32 devices in a mesh: grp: 2 (over y), sp: 4 (over z), tp: 4 (over x, core).
Axes of the slice: x: 2, y: 2, z: 4, core: 2. Of those that a mesh axis runs over, the one named last changes fastest.
Arguments:
- layer_input: bfloat16 [8, 1536, 2048], P(('grp', 'tp'), 'sp'), parts along dimension 0, may hold values from -6 to 6
- input_gain: float32 [2048], replicated, may hold values from 0.1 to 1.9
- key_weight: bfloat16 [2048, 512], replicated, may hold values from -0.125 to 0.125
- value_weight: bfloat16 [2048, 512], replicated, may hold values from -0.125 to 0.125
- stick_offsets: bfloat16 [4, 8, 1536], P(None, ('grp', 'tp'), 'sp'), parts along dimension 1
- head_bias: float32 [16], replicated
- queries: bfloat16 [8, 4, 512], P(('grp', 'tp'), 'sp'), parts along dimension 0, may hold values from -6 to 6
Outputs:
- key_cache: bfloat16 [8, 4, 1536, 128], P(('grp', 'tp'), 'sp'), parts along dimension 0
- value_cache: bfloat16 [8, 4, 1536, 128], P(('grp', 'tp'), 'sp'), parts along dimension 0
- offset_cache: bfloat16 [8, 4, 1536], P(('grp', 'tp'), 'sp'), parts along dimension 0
- first_read: bfloat16 [8, 4, 512], P(('grp', 'tp'), 'sp'), parts along dimension 0
The draws below stay inside these ranges and needn't reach their ends.
There are 2 independent parts, one for each index of `grp`. The reference program is written for one: setup_inputs(seed, part) draws one part's arguments, and reference() takes and returns one part's arrays. A program takes and returns all parts, laid end to end along the dimension named above; an argument that names none is the same for every part. Nothing has to cross between parts.
All inputs are finite; a program needn't handle non-finite values.
Results may differ from the reference program's by a relative error of at most 0.014.
Values may be sent and summed in bfloat16 or wider, within the bound.
A program may use at most 64 MiB of HBM per device.

```python
import math
import jax
import jax.numpy as jnp
from jax import lax

D = 2048
H = 16
KVH = 4
HD = 128
BLOCK = 384
QG = 4
SEQS = 4
LEN = 1536
N_SP = 4
N_TP = 4


def draw_head_bias(key, part):
    pick_key = jax.random.fold_in(key, 11)
    slow_key = jax.random.fold_in(key, 12)
    fast_key = jax.random.fold_in(key, 13)
    fast_share = 0.5
    fast_heads = jax.random.bernoulli(pick_key, fast_share, (H,))
    slow_value = -math.log(LEN) - jax.random.uniform(slow_key, (H,), jnp.float32, 0.5, 1.5)
    fast_value = -4.0 + jax.random.uniform(fast_key, (H,), jnp.float32, -0.5, 0.5)
    return jnp.where(fast_heads, fast_value, slow_value).astype(jnp.float32)


def draw_stick_offsets(key, part):
    level_key = jax.random.fold_in(key, 21)
    jitter_key = jax.random.fold_in(key, 22)
    place_key = jax.random.fold_in(key, 23)
    height_key = jax.random.fold_in(key, 24)
    level_range = 0.7
    blocks = LEN // BLOCK
    tier_entries = jax.random.uniform(level_key, (KVH, SEQS, blocks), jnp.float32, -level_range, level_range)
    tier_entries = jnp.repeat(tier_entries, BLOCK, axis=2)
    stochastic_jitter = jnp.clip(0.3 * jax.random.normal(jitter_key, (KVH, SEQS, LEN), jnp.float32), -1.0, 1.0)
    slot_destinations = jax.random.randint(place_key, (KVH, SEQS, 2), 0, LEN)
    vertical_extent_entries = math.log(LEN) + jax.random.uniform(height_key, (KVH, SEQS, 2), jnp.float32, 0.0, 1.0)
    sequence_slot_index = jnp.arange(LEN)
    clustered_sets = jnp.sum(jnp.where(sequence_slot_index[None, None, None, :] == slot_destinations[..., None], vertical_extent_entries[..., None], 0.0), axis=2)
    return (tier_entries + stochastic_jitter + clustered_sets).astype(jnp.bfloat16)


def level_of(stream_key, shape, cuts, least, top_value):
    def one(position, blocks):
        steps = jax.random.uniform(jax.random.fold_in(jax.random.fold_in(stream_key, 6), position), (blocks,), jnp.float32, least / len(cuts), top_value / len(cuts))
        return jnp.repeat(jnp.exp(steps), shape[position] // blocks).reshape((-1,) + (1,) * (len(shape) - position - 1))

    loudness = one(*cuts[0])
    for cut in cuts[1:]:
        loudness = loudness * one(*cut)
    return loudness


def normal_values(stream_key, dims, scale, bound, split=(), held_as=jnp.bfloat16):
    entries = jax.random.normal(stream_key, dims, jnp.float32) * scale
    if len(split) > 0:
        entries = level_of(stream_key, dims, split, -0.22, 0.18) * entries
    return jnp.clip(entries, min=-bound, max=bound).astype(held_as)


def setup_inputs(seed: int = 0, part: int = 0) -> dict:
    seeds = jax.random.split(jax.random.key(seed), 8)
    part_splits = jax.random.split(jax.random.fold_in(seeds[7], part), 8)
    return {
        "layer_input": normal_values(part_splits[0], (SEQS, LEN, D), 1.0, 6.0, ((0, 4), (1, 4))),
        "input_gain": jnp.clip(1.0 + 0.18 * jax.random.normal(seeds[1], (D,), jnp.float32), 0.1, 1.9),
        "key_weight": normal_values(seeds[2], (D, KVH * HD), D ** -0.5, 0.125),
        "value_weight": normal_values(seeds[3], (D, KVH * HD), D ** -0.5, 0.125),
        "stick_offsets": draw_stick_offsets(jax.random.fold_in(jax.random.fold_in(seeds[7], part), 71), part),
        "head_bias": draw_head_bias(jax.random.fold_in(seeds[7], 71), part),
        "queries": normal_values(part_splits[6], (N_TP, N_SP, QG * HD), 1.0, 6.0, ((0, 4), (1, 4))),
    }


EPSILON = 1e-06

def rms_scale(matrix):
    return matrix * lax.rsqrt(lax.optimization_barrier(jnp.mean(matrix * matrix, axis=-1, keepdims=True)) + EPSILON)

def stick_weights(scores, spread, carried):
    inside = lax.cumsum(spread, axis=scores.ndim - 1, reverse=True) - spread
    return jnp.exp(jax.nn.log_sigmoid(scores) - inside - carried)

def reference(layer_input, input_gain, key_weight, value_weight, stick_offsets, head_bias, queries):
    group_size = H // KVH
    per_column = N_SP // KVH

    def one_sequence(tokens):
        widened = tokens.astype(jnp.float32)
        normed_rows = (rms_scale(widened) * input_gain).astype(jnp.bfloat16)
        key_rows = jnp.dot(normed_rows, key_weight, preferred_element_type=jnp.float32).astype(jnp.bfloat16)
        value_rows = jnp.dot(normed_rows, value_weight, preferred_element_type=jnp.float32).astype(jnp.bfloat16)
        return (key_rows, value_rows)
    key_rows, value_rows = lax.map(one_sequence, layer_input)
    key_cache = jnp.transpose(key_rows.reshape(N_TP, per_column, LEN, KVH, HD), (0, 1, 3, 2, 4)).reshape(N_TP, N_SP, LEN, HD)
    value_cache = jnp.transpose(value_rows.reshape(N_TP, per_column, LEN, KVH, HD), (0, 1, 3, 2, 4)).reshape(N_TP, N_SP, LEN, HD)
    offset_cache = jnp.transpose(stick_offsets.reshape(KVH, N_TP, per_column, LEN), (1, 2, 0, 3)).reshape(N_TP, N_SP, LEN)
    bias_all = jnp.tile(head_bias.reshape(KVH, group_size), (N_TP * per_column, 1))

    def one_read(pieces):
        query_row, key_block, value_block, offset_row, bias_row = pieces
        scores = jnp.dot(query_row.reshape(group_size, HD), key_block.T, preferred_element_type=jnp.float32)
        scores = scores / math.sqrt(HD) + bias_row[:, None] + offset_row.astype(jnp.float32)[None, :]
        spread = jax.nn.softplus(scores)
        weights = stick_weights(scores, spread, 0.0).astype(jnp.bfloat16)
        mixture = jnp.dot(weights, value_block, preferred_element_type=jnp.float32)
        return rms_scale(mixture).astype(jnp.bfloat16).reshape(group_size * HD)
    first_read = lax.map(one_read, (queries.reshape(N_TP * N_SP, group_size * HD), key_cache.reshape(N_TP * N_SP, LEN, HD), value_cache.reshape(N_TP * N_SP, LEN, HD), offset_cache.reshape(N_TP * N_SP, LEN), bias_all))
    return (key_cache, value_cache, offset_cache, first_read.reshape(N_TP, N_SP, group_size * HD))
```

```python
import functools
import math

import jax
import jax.numpy as jnp
from jax import lax
from jax.experimental import pallas as pl
from jax.experimental.pallas import tpu as pltpu
from jax.sharding import PartitionSpec as P

H = 16
KVH = 4
HD = 128
GROUP = H // KVH
EPSILON = 1e-06
ROWS = 128
FIRST = 64
STEP = 16
VMEM_BYTES = 67043328
SPARE_BYTES = 524288
WRITE_BYTES = 1048576
MESH = pl.DeviceIdType.MESH


def last_source(me, n):
    return jnp.where(2 * me < n, n // 2, n // 2 - 1)


def kernel(
    n, seqs, chunks, x_hbm, gain_hbm, wk_hbm, wv_hbm, off_hbm, bias_hbm, q_hbm,
    k_land, v_land, off_out, stick, mix_out,
    x_buf, scaled, row_scale, weights, sends, gain_buf, bias_buf, off_in, off_send, off_land, q_buf,
    x_sem, w_sem, small_sem, k_sem, v_sem, o_sem,
):
    total, width = x_buf.shape
    block = total // seqs
    length = n * block
    me = lax.axis_index("sp")
    order = range(1, n)
    lower = 2 * me < n
    near = jnp.where(lower, me, n - 1 - me)

    barrier = pltpu.get_barrier_semaphore()
    for d in order:
        pl.semaphore_signal(
            barrier, inc=1, device_id={"sp": lax.rem(me + d, n)}, device_id_type=MESH
        )

    def peer(i):
        if i == 0:
            return me
        far = jnp.where(i <= n - 1 - near, n - i, n - 1 - i)
        return jnp.where(lower, far, n - 1 - far)

    def offset(i):
        return lax.rem(peer(i) - me + n, n)

    def head_of(i):
        return lax.rem(peer(i), KVH)

    x_copies = []
    for c, (start, rows) in enumerate(chunks):
        part = pl.ds(start, rows)
        x_copies.append(pltpu.make_async_copy(x_hbm.at[part], x_buf.at[part], x_sem.at[c]))
    w_copies = []
    for j in range(KVH):
        h = head_of((j + 1) % n)
        columns = pl.ds(pl.multiple_of(h * HD, HD), HD)
        for kind, w_hbm in enumerate((wk_hbm, wv_hbm)):
            w_copies.append(pltpu.make_async_copy(
                w_hbm.at[:, columns], weights.at[h, :, pl.ds(kind * HD, HD)], w_sem.at[j, kind]
            ))
    gain_copy = pltpu.make_async_copy(gain_hbm, gain_buf, small_sem.at[0])
    off_copy = pltpu.make_async_copy(off_hbm, off_in, small_sem.at[1])
    q_copy = pltpu.make_async_copy(q_hbm, q_buf, small_sem.at[2])
    bias_copy = pltpu.make_async_copy(bias_hbm, bias_buf, small_sem.at[3])
    gain_copy.start()
    x_copies[0].start()
    w_copies[0].start()
    w_copies[1].start()
    for copy in x_copies[1:]:
        copy.start()
    for copy in w_copies[2:]:
        copy.start()
    off_copy.start()
    q_copy.start()
    bias_copy.start()

    gain_copy.wait()
    gain = gain_buf[...]

    def prepare(c):
        start, count = chunks[c]
        x_copies[c].wait()

        def step(i, _):
            rows = pl.ds(pl.multiple_of(start + i * STEP, STEP), STEP)
            x = x_buf[rows, :].astype(jnp.float32)
            scaled[rows, :] = (x * gain).astype(jnp.bfloat16)
            scale = lax.rsqrt(jnp.mean(x * x, axis=-1, keepdims=True) + EPSILON)
            row_scale[rows, :] = jnp.broadcast_to(scale, (STEP, HD))
            return 0

        lax.fori_loop(0, count // STEP, step, 0, unroll=4)

    def wait_weights(i):
        j = (i - 1) % n
        if j < KVH:
            w_copies[2 * j].wait()
            w_copies[2 * j + 1].wait()

    def project(i, start, count):
        base = lax.div(peer(i), KVH) * block if seqs > 1 else 0
        rows = pl.ds(pl.multiple_of(base + start, STEP) if seqs > 1 else start, count)
        both = jnp.dot(
            scaled[rows, :], weights[head_of(i)], preferred_element_type=jnp.float32
        )
        scale = row_scale[rows, :]
        return [
            (both[:, kind * HD:(kind + 1) * HD] * scale).astype(jnp.bfloat16) for kind in range(2)
        ]

    lands = ((k_land, k_sem), (v_land, v_sem))

    def remote(src, dst, sem, d, target):
        return pltpu.make_async_remote_copy(
            src_ref=src, dst_ref=dst, send_sem=sem.at[0, d], recv_sem=sem.at[1, d],
            device_id={"sp": target}, device_id_type=MESH,
        )

    def block_copy(kind, i, start=0, count=block):
        land, sem = lands[kind]
        there = pl.ds(pl.multiple_of(me * block + start, STEP), count)
        return remote(
            sends.at[kind, i, pl.ds(start, count)], land.at[0, 0, there], sem, offset(i), peer(i)
        )

    def offset_copy(i):
        return remote(off_send.at[peer(i)], off_land.at[me], o_sem, offset(i), peer(i))

    def send(i, start, count):
        for kind, values in enumerate(project(i, start, count)):
            sends[kind, i, pl.ds(start, count)] = values
        if i == 1 and start == 0:
            pl.semaphore_wait(barrier, n - 1)
        for kind in range(2):
            block_copy(kind, i, start, count).start()

    if seqs == 1:
        for c, (start, count) in enumerate(chunks):
            prepare(c)
            if c == 0:
                wait_weights(1)
            send(1, start, count)
    else:
        for c in range(len(chunks)):
            prepare(c)
        wait_weights(1)
        send(1, 0, block)
    off_copy.wait()
    for s in range(seqs):
        values = off_in[s].astype(jnp.float32)
        for h in range(KVH):
            off_send[s * KVH + h] = values[h:h + 1, :]
    off_land[me] = off_send[me]
    for i in order:
        offset_copy(i).start()
    for i in order[1:]:
        wait_weights(i)
        send(i, 0, block)
    wait_weights(0)
    here = pl.ds(pl.multiple_of(me * block, block), block)
    for (land, _), values in zip(lands, project(0, 0, block)):
        land[0, 0, here] = values

    def rows_of(source):
        return pl.ds(pl.multiple_of(source * block, block), block)

    def arrived(kind, source):
        land, sem = lands[kind]
        d = lax.rem(me - source + n, n)
        remote(
            sends.at[kind, 0], land.at[0, 0, rows_of(source)], sem, d, source
        ).wait_recv()

    q_copy.wait()
    q_all = q_buf[0].astype(jnp.float32)
    q_rows = jnp.concatenate([q_all[:, g * HD:(g + 1) * HD] for g in range(GROUP)] * 2, axis=0)
    q_rows = q_rows.astype(jnp.bfloat16)
    bias_copy.wait()
    row_id = lax.broadcasted_iota(jnp.int32, (2 * GROUP, H), 0)
    lane_id = lax.broadcasted_iota(jnp.int32, (2 * GROUP, H), 1)
    chosen = lane_id == lax.rem(me, KVH) * GROUP + lax.rem(row_id, GROUP)
    bias = jnp.sum(jnp.where(chosen, bias_buf[...], 0.0), axis=1, keepdims=True)
    for d in order:
        source = lax.rem(me + n - d, n)
        remote(off_send.at[0], off_land.at[source], o_sem, d, source).wait_recv()
    off_row = jnp.concatenate([off_land[i] for i in range(n)], axis=1)
    off_out[0] = off_row.astype(jnp.bfloat16)

    last = last_source(me, n)

    def source_of(j):
        start = lax.rem(last + 1 + j, n)
        return start

    sources = [source_of(j) for j in range(n - 1)]

    def wait_block(kind, source):
        @pl.when(source != me)
        def _():
            arrived(kind, source)

    for source in sources:
        wait_block(0, source)
    arrived(0, last)
    scores = lax.dot_general(
        q_rows, k_land[0, 0], (((1,), (1,)), ((), ())), preferred_element_type=jnp.float32
    )
    scores = scores / math.sqrt(HD) + bias + off_row
    tail = jnp.log1p(jnp.exp(-jnp.abs(scores)))
    spread = jnp.maximum(scores, 0.0) + tail
    log_sig = jnp.minimum(scores, 0.0) - tail
    pieces = length // HD
    cut = [spread[:, c * HD:(c + 1) * HD] for c in range(pieces)]
    stacked = jnp.concatenate(cut, axis=0)
    after = (
        lax.broadcasted_iota(jnp.int32, (HD, HD), 0) > lax.broadcasted_iota(jnp.int32, (HD, HD), 1)
    ).astype(jnp.float32)
    inner = jnp.dot(
        stacked, after, preferred_element_type=jnp.float32, precision=lax.Precision.HIGHEST
    )
    sums = jnp.sum(stacked, axis=1, keepdims=True)
    carried = jnp.zeros((2 * GROUP, 1), jnp.float32)
    for c in reversed(range(pieces)):
        rows = slice(c * 2 * GROUP, (c + 1) * 2 * GROUP)
        beyond = inner[rows] + carried
        stick[:, c * HD:(c + 1) * HD] = jnp.exp(log_sig[:, c * HD:(c + 1) * HD] - beyond)
        carried = carried + sums[rows]

    mixture = jnp.zeros((2 * GROUP, HD), jnp.float32)
    for source in sources:
        wait_block(1, source)
        part = rows_of(source)
        mixture = mixture + jnp.dot(
            stick[:, part].astype(jnp.bfloat16), v_land[0, 0, part, :],
            preferred_element_type=jnp.float32,
        )
    mix_out[...] = mixture
    for i in order:
        block_copy(0, i).wait_send()
        block_copy(1, i).wait_send()
        offset_copy(i).wait_send()
    arrived(1, last)


def finish(
    n, k_in, v_in, off_in, stick_in, mix_in, k_out, v_out, off_out, read_out, read_buf, sem
):
    copies = [
        pltpu.make_async_copy(src, dst, sem.at[i])
        for i, (src, dst) in enumerate(((k_in, k_out), (v_in, v_out), (off_in, off_out)))
    ]
    for copy in copies:
        copy.start()
    block = v_in.shape[2] // n
    last = last_source(lax.axis_index("sp"), n)
    part = pl.ds(pl.multiple_of(last * block, block), block)
    mixture = mix_in[...] + jnp.dot(
        stick_in[:, part].astype(jnp.bfloat16), v_in[0, 0, part, :],
        preferred_element_type=jnp.float32,
    )
    scale = lax.rsqrt(jnp.mean(mixture * mixture, axis=-1, keepdims=True) + EPSILON)
    read = mixture * scale
    read_buf[0] = jnp.concatenate([read[g:g + 1] for g in range(GROUP)], axis=1).astype(jnp.bfloat16)
    copies.append(pltpu.make_async_copy(read_buf, read_out, sem.at[3]))
    copies[3].start()
    for copy in copies:
        copy.wait()


def chunks_of(seqs, block):
    if seqs > 1:
        return tuple((r, ROWS) for r in range(0, seqs * block, ROWS))
    return ((0, FIRST), (FIRST, ROWS), (FIRST + ROWS, block - FIRST - ROWS))


def shards(layer_input, input_gain, key_weight, value_weight, stick_offsets, head_bias, queries):
    seqs, block, width = layer_input.shape
    n = lax.axis_size("sp")
    length = n * block
    total = seqs * block
    hbm = pl.BlockSpec(memory_space=pltpu.HBM)
    vmem = pl.BlockSpec(memory_space=pltpu.VMEM)
    group_width = queries.shape[-1]
    chunks = chunks_of(seqs, block)
    cache = ((1, 1, length, HD), jnp.bfloat16)
    offsets = ((1, 1, length), jnp.bfloat16)
    read = ((1, 1, group_width), jnp.bfloat16)
    held_outs = (
        cache,
        cache,
        offsets,
        ((2 * GROUP, length), jnp.float32),
        ((2 * GROUP, HD), jnp.float32),
    )
    held = pl.pallas_call(
        functools.partial(kernel, n, seqs, chunks),
        out_shape=tuple(pltpu.VMEM(*out) for out in held_outs),
        in_specs=[hbm] * 7,
        out_specs=(vmem,) * len(held_outs),
        scratch_shapes=[
            pltpu.VMEM((total, width), jnp.bfloat16),
            pltpu.VMEM((total, width), jnp.bfloat16),
            pltpu.VMEM((total, HD), jnp.float32),
            pltpu.VMEM((KVH, width, 2 * HD), jnp.bfloat16),
            pltpu.VMEM((2, n, block, HD), jnp.bfloat16),
            pltpu.VMEM((1, width), jnp.float32),
            pltpu.VMEM((1, H), jnp.float32),
            pltpu.VMEM((seqs, KVH, block), jnp.bfloat16),
            pltpu.VMEM((n, 1, block), jnp.float32),
            pltpu.VMEM((n, 1, block), jnp.float32),
            pltpu.VMEM((1, 1, group_width), jnp.bfloat16),
            pltpu.SemaphoreType.DMA((len(chunks),)),
            pltpu.SemaphoreType.DMA((KVH, 2)),
            pltpu.SemaphoreType.DMA((4,)),
            pltpu.SemaphoreType.DMA((2, n)),
            pltpu.SemaphoreType.DMA((2, n)),
            pltpu.SemaphoreType.DMA((2, n)),
        ],
        compiler_params=pltpu.CompilerParams(
            collective_id=0, has_side_effects=True, vmem_limit_bytes=VMEM_BYTES - 4 * length * HD - SPARE_BYTES
        ),
    )(
        layer_input.reshape(total, width),
        input_gain.reshape(1, width),
        key_weight,
        value_weight,
        jnp.transpose(stick_offsets, (1, 0, 2)),
        head_bias.reshape(1, H),
        queries,
    )
    outs = (cache, cache, offsets, read)
    return pl.pallas_call(
        functools.partial(finish, n),
        out_shape=tuple(jax.ShapeDtypeStruct(*out) for out in outs),
        in_specs=[vmem] * len(held_outs),
        out_specs=(hbm,) * len(outs),
        scratch_shapes=[
            pltpu.VMEM(*read),
            pltpu.SemaphoreType.DMA((len(outs),)),
        ],
        compiler_params=pltpu.CompilerParams(vmem_limit_bytes=WRITE_BYTES),
    )(*held)


def solution(mesh):
    placed = (
        P(("grp", "tp"), "sp", None),
        P(),
        P(),
        P(),
        P(None, ("grp", "tp"), "sp"),
        P(),
        P(("grp", "tp"), "sp", None),
    )
    return jax.shard_map(
        shards,
        mesh=mesh,
        in_specs=placed,
        out_specs=(
            P(("grp", "tp"), "sp", None, None),
            P(("grp", "tp"), "sp", None, None),
            P(("grp", "tp"), "sp", None),
            P(("grp", "tp"), "sp", None),
        ),
        check_vma=False,
    )
```

```python
import functools
import math

import jax
import jax.numpy as jnp
from jax import lax
from jax.experimental import pallas as pl
from jax.experimental.pallas import tpu as pltpu
from jax.sharding import PartitionSpec as P

H = 16
KVH = 4
HD = 128
GROUP = H // KVH
EPSILON = 1e-06
ROWS = 128
FIRST = 128
STEP = 16
VMEM_BYTES = 67043328
SPARE_BYTES = 524288
WRITE_BYTES = 1048576
MESH = pl.DeviceIdType.MESH


def last_source(me, n):
    return jnp.where(2 * me < n, n // 2, n // 2 - 1)


def kernel(
    n, seqs, chunks, x_hbm, gain_hbm, wk_hbm, wv_hbm, off_hbm, bias_hbm, q_hbm,
    k_land, v_land, off_out, stick, mix_out,
    x_buf, scaled, row_scale, weights, sends, gain_buf, bias_buf, off_in, off_send, off_land, q_buf,
    x_sem, w_sem, small_sem, send_sem, k_sem, v_sem, o_sem,
):
    total, width = x_buf.shape
    block = total // seqs
    length = n * block
    me = lax.axis_index("sp")
    order = range(1, n)
    lower = 2 * me < n
    near = jnp.where(lower, me, n - 1 - me)

    def peer(i):
        if i == 0:
            return me
        far = jnp.where(i <= n - 1 - near, n - i, n - 1 - i)
        return jnp.where(lower, far, n - 1 - far)

    def head_of(i):
        return lax.rem(peer(i), KVH)

    x_copies = []
    for c, (start, rows) in enumerate(chunks):
        part = pl.ds(start, rows)
        x_copies.append(pltpu.make_async_copy(x_hbm.at[part], x_buf.at[part], x_sem.at[c]))
    w_copies = []
    for j in range(KVH):
        columns = pl.ds(pl.multiple_of(head_of((j + 1) % n) * HD, HD), HD)
        for kind, w_hbm in enumerate((wk_hbm, wv_hbm)):
            w_copies.append(pltpu.make_async_copy(
                w_hbm.at[:, columns],
                weights.at[j, :, pl.ds(kind * HD, HD)],
                w_sem.at[min(j, 1)],
            ))
    gain_copy = pltpu.make_async_copy(gain_hbm, gain_buf, small_sem.at[0])
    off_copy = pltpu.make_async_copy(off_hbm, off_in, small_sem.at[1])
    q_copy = pltpu.make_async_copy(q_hbm, q_buf, small_sem.at[2])
    bias_copy = pltpu.make_async_copy(bias_hbm, bias_buf, small_sem.at[3])
    gain_copy.start()
    x_copies[0].start()
    w_copies[0].start()
    w_copies[1].start()
    for copy in x_copies[1:]:
        copy.start()
    barrier = pltpu.get_barrier_semaphore()
    for d in order:
        pl.semaphore_signal(
            barrier, inc=1, device_id={"sp": lax.rem(me + d, n)}, device_id_type=MESH
        )

    gain_copy.wait()
    gain = gain_buf[...]

    def prepare(c):
        start, count = chunks[c]
        x_copies[c].wait()

        def step(i, _):
            rows = pl.ds(pl.multiple_of(start + i * STEP, STEP), STEP)
            x = x_buf[rows, :].astype(jnp.float32)
            scaled[rows, :] = (x * gain).astype(jnp.bfloat16)
            scale = lax.rsqrt(jnp.mean(x * x, axis=-1, keepdims=True) + EPSILON)
            row_scale[rows, :] = jnp.broadcast_to(scale, (STEP, HD))
            return 0

        lax.fori_loop(0, count // STEP, step, 0, unroll=4)

    def wait_weights(i):
        if i == 1:
            part = weights.at[pl.ds(0, 1)]
            pltpu.make_async_copy(part, part, w_sem.at[0]).wait()
            for copy in w_copies[2:]:
                copy.start()
            off_copy.start()
            q_copy.start()
            bias_copy.start()
        if i == 2 % n:
            part = weights.at[pl.ds(1, KVH - 1)]
            pltpu.make_async_copy(part, part, w_sem.at[1]).wait()

    def slot(i):
        if n == KVH:
            return (i - 1) % n
        first = head_of(1)
        down = lax.rem(first - head_of(i) + KVH, KVH)
        return jnp.where(lower, down, lax.rem(KVH - down, KVH))

    def project(i, start, count):
        base = lax.div(peer(i), KVH) * block if seqs > 1 else 0
        rows = pl.ds(pl.multiple_of(base + start, STEP) if seqs > 1 else start, count)
        both = jnp.dot(
            scaled[rows, :], weights[slot(i)], preferred_element_type=jnp.float32
        )
        scale = row_scale[rows, :]
        return [
            (both[:, kind * HD:(kind + 1) * HD] * scale).astype(jnp.bfloat16) for kind in range(2)
        ]

    lands = (k_land, v_land)

    def remote(src, dst, sent, landed, target):
        return pltpu.make_async_remote_copy(
            src_ref=src, dst_ref=dst, send_sem=send_sem.at[sent], recv_sem=landed,
            device_id={"sp": target}, device_id_type=MESH,
        )

    def landed_sem(kind, source, target):
        if kind == 0:
            return k_sem.at[0]
        return v_sem.at[jnp.where(source == last_source(target, n), 1, 0)]

    def block_copy(kind, i, start, count):
        there = pl.ds(pl.multiple_of(me * block + start, STEP), count)
        return remote(
            sends.at[i - 1, kind, pl.ds(start, count)],
            lands[kind].at[0, 0, there],
            0,
            landed_sem(kind, me, peer(i)),
            peer(i),
        )

    def offset_copy(i):
        return remote(off_send.at[peer(i)], off_land.at[me], 1, o_sem.at[0], peer(i))

    def send(i, start, count):
        for kind, values in enumerate(project(i, start, count)):
            sends[i - 1, kind, pl.ds(start, count)] = values
        if i == 1 and start == 0:
            pl.semaphore_wait(barrier, n - 1)
        for kind in range(2):
            block_copy(kind, i, start, count).start()

    if seqs == 1:
        for c, (start, count) in enumerate(chunks):
            prepare(c)
            if c == 0:
                wait_weights(1)
            send(1, start, count)
    else:
        for c in range(len(chunks)):
            prepare(c)
        wait_weights(1)
        send(1, 0, block)
    off_copy.wait()
    for s in range(seqs):
        values = off_in[s].astype(jnp.float32)
        for h in range(KVH):
            off_send[s * KVH + h] = values[h:h + 1, :]
    off_land[me] = off_send[me]
    for i in order:
        offset_copy(i).start()
    for i in order[1:]:
        wait_weights(i)
        send(i, 0, block)
    wait_weights(0)
    here = pl.ds(pl.multiple_of(me * block, block), block)
    for land, values in zip(lands, project(0, 0, block)):
        land[0, 0, here] = values

    def rows_of(source):
        return pl.ds(pl.multiple_of(source * block, block), block)

    def arrived(kind, blocks, sem):
        part = lands[kind].at[0, 0, pl.ds(0, blocks * block)]
        remote(part, part, 0, sem, peer(1)).wait_recv()

    q_copy.wait()
    q_all = q_buf[0].astype(jnp.float32)
    q_rows = jnp.concatenate([q_all[:, g * HD:(g + 1) * HD] for g in range(GROUP)] * 2, axis=0)
    q_rows = q_rows.astype(jnp.bfloat16)
    bias_copy.wait()
    row_id = lax.broadcasted_iota(jnp.int32, (2 * GROUP, H), 0)
    lane_id = lax.broadcasted_iota(jnp.int32, (2 * GROUP, H), 1)
    chosen = lane_id == lax.rem(me, KVH) * GROUP + lax.rem(row_id, GROUP)
    bias = jnp.sum(jnp.where(chosen, bias_buf[...], 0.0), axis=1, keepdims=True)
    part = off_land.at[pl.ds(0, n - 1)]
    remote(part, part, 1, o_sem.at[0], peer(1)).wait_recv()
    off_row = jnp.concatenate([off_land[i] for i in range(n)], axis=1)
    off_out[0] = off_row.astype(jnp.bfloat16)

    last = last_source(me, n)

    arrived(0, n - 1, k_sem.at[0])
    scores = lax.dot_general(
        q_rows, k_land[0, 0], (((1,), (1,)), ((), ())), preferred_element_type=jnp.float32
    )
    scores = scores / math.sqrt(HD) + bias + off_row
    tail = jnp.log1p(jnp.exp(-jnp.abs(scores)))
    spread = jnp.maximum(scores, 0.0) + tail
    log_sig = jnp.minimum(scores, 0.0) - tail
    pieces = length // HD
    cut = [spread[:, c * HD:(c + 1) * HD] for c in range(pieces)]
    stacked = jnp.concatenate(cut, axis=0)
    after = (
        lax.broadcasted_iota(jnp.int32, (HD, HD), 0) > lax.broadcasted_iota(jnp.int32, (HD, HD), 1)
    ).astype(jnp.float32)
    inner = jnp.dot(
        stacked, after, preferred_element_type=jnp.float32, precision=lax.Precision.HIGHEST
    )
    sums = jnp.sum(stacked, axis=1, keepdims=True)
    carried = jnp.zeros((2 * GROUP, 1), jnp.float32)
    for c in reversed(range(pieces)):
        rows = slice(c * 2 * GROUP, (c + 1) * 2 * GROUP)
        beyond = inner[rows] + carried
        stick[:, c * HD:(c + 1) * HD] = jnp.exp(log_sig[:, c * HD:(c + 1) * HD] - beyond)
        carried = carried + sums[rows]

    if n > 2:
        arrived(1, n - 2, v_sem.at[0])
    mixture = jnp.zeros((2 * GROUP, HD), jnp.float32)
    for j in range(n - 1):
        part = rows_of(lax.rem(last + 1 + j, n))
        mixture = mixture + jnp.dot(
            stick[:, part].astype(jnp.bfloat16), v_land[0, 0, part, :],
            preferred_element_type=jnp.float32,
        )
    mix_out[...] = mixture
    remote(sends, sends, 0, k_sem.at[0], peer(1)).wait_send()
    part = off_send.at[pl.ds(0, n - 1)]
    remote(part, part, 1, o_sem.at[0], peer(1)).wait_send()
    arrived(1, 1, v_sem.at[1])


def finish(
    n, k_in, v_in, off_in, stick_in, mix_in, k_out, v_out, off_out, read_out, read_buf, sem
):
    copies = [
        pltpu.make_async_copy(src, dst, sem.at[i])
        for i, (src, dst) in enumerate(((k_in, k_out), (v_in, v_out), (off_in, off_out)))
    ]
    for copy in copies:
        copy.start()
    block = v_in.shape[2] // n
    last = last_source(lax.axis_index("sp"), n)
    part = pl.ds(pl.multiple_of(last * block, block), block)
    mixture = mix_in[...] + jnp.dot(
        stick_in[:, part].astype(jnp.bfloat16), v_in[0, 0, part, :],
        preferred_element_type=jnp.float32,
    )
    scale = lax.rsqrt(jnp.mean(mixture * mixture, axis=-1, keepdims=True) + EPSILON)
    read = mixture * scale
    read_buf[0] = jnp.concatenate([read[g:g + 1] for g in range(GROUP)], axis=1).astype(jnp.bfloat16)
    copies.append(pltpu.make_async_copy(read_buf, read_out, sem.at[3]))
    copies[3].start()
    for copy in copies:
        copy.wait()


def chunks_of(seqs, block):
    if seqs > 1:
        return tuple((r, ROWS) for r in range(0, seqs * block, ROWS))
    return ((0, FIRST), (FIRST, block - FIRST))


def shards(layer_input, input_gain, key_weight, value_weight, stick_offsets, head_bias, queries):
    seqs, block, width = layer_input.shape
    n = lax.axis_size("sp")
    length = n * block
    total = seqs * block
    hbm = pl.BlockSpec(memory_space=pltpu.HBM)
    vmem = pl.BlockSpec(memory_space=pltpu.VMEM)
    group_width = queries.shape[-1]
    chunks = chunks_of(seqs, block)
    cache = ((1, 1, length, HD), jnp.bfloat16)
    offsets = ((1, 1, length), jnp.bfloat16)
    read = ((1, 1, group_width), jnp.bfloat16)
    held_outs = (
        cache,
        cache,
        offsets,
        ((2 * GROUP, length), jnp.float32),
        ((2 * GROUP, HD), jnp.float32),
    )
    held = pl.pallas_call(
        functools.partial(kernel, n, seqs, chunks),
        out_shape=tuple(pltpu.VMEM(*out) for out in held_outs),
        in_specs=[hbm] * 7,
        out_specs=(vmem,) * len(held_outs),
        scratch_shapes=[
            pltpu.VMEM((total, width), jnp.bfloat16),
            pltpu.VMEM((total, width), jnp.bfloat16),
            pltpu.VMEM((total, HD), jnp.float32),
            pltpu.VMEM((KVH, width, 2 * HD), jnp.bfloat16),
            pltpu.VMEM((n - 1, 2, block, HD), jnp.bfloat16),
            pltpu.VMEM((1, width), jnp.float32),
            pltpu.VMEM((1, H), jnp.float32),
            pltpu.VMEM((seqs, KVH, block), jnp.bfloat16),
            pltpu.VMEM((n, 1, block), jnp.float32),
            pltpu.VMEM((n, 1, block), jnp.float32),
            pltpu.VMEM((1, 1, group_width), jnp.bfloat16),
            pltpu.SemaphoreType.DMA((len(chunks),)),
            pltpu.SemaphoreType.DMA((2,)),
            pltpu.SemaphoreType.DMA((4,)),
            pltpu.SemaphoreType.DMA((2,)),
            pltpu.SemaphoreType.DMA((1,)),
            pltpu.SemaphoreType.DMA((2,)),
            pltpu.SemaphoreType.DMA((1,)),
        ],
        compiler_params=pltpu.CompilerParams(
            collective_id=0, has_side_effects=True, vmem_limit_bytes=VMEM_BYTES - 4 * length * HD - SPARE_BYTES
        ),
    )(
        layer_input.reshape(total, width),
        input_gain.reshape(1, width),
        key_weight,
        value_weight,
        jnp.transpose(stick_offsets, (1, 0, 2)),
        head_bias.reshape(1, H),
        queries,
    )
    outs = (cache, cache, offsets, read)
    return pl.pallas_call(
        functools.partial(finish, n),
        out_shape=tuple(jax.ShapeDtypeStruct(*out) for out in outs),
        in_specs=[vmem] * len(held_outs),
        out_specs=(hbm,) * len(outs),
        scratch_shapes=[
            pltpu.VMEM(*read),
            pltpu.SemaphoreType.DMA((len(outs),)),
        ],
        compiler_params=pltpu.CompilerParams(vmem_limit_bytes=WRITE_BYTES),
    )(*held)


def solution(mesh):
    placed = (
        P(("grp", "tp"), "sp", None),
        P(),
        P(),
        P(),
        P(None, ("grp", "tp"), "sp"),
        P(),
        P(("grp", "tp"), "sp", None),
    )
    return jax.shard_map(
        shards,
        mesh=mesh,
        in_specs=placed,
        out_specs=(
            P(("grp", "tp"), "sp", None, None),
            P(("grp", "tp"), "sp", None, None),
            P(("grp", "tp"), "sp", None),
            P(("grp", "tp"), "sp", None),
        ),
        check_vma=False,
    )
```

```python
import functools
import math

import jax
import jax.numpy as jnp
from jax import lax
from jax.experimental import pallas as pl
from jax.experimental.pallas import tpu as pltpu
from jax.sharding import PartitionSpec as P

H = 16
KVH = 4
HD = 128
GROUP = H // KVH
EPSILON = 1e-06
ROWS = 128
STEP = 16
TILE = 8
DEPTH = 256
VMEM_BYTES = 67043328
SPARE_BYTES = 524288
WRITE_BYTES = 1048576
MESH = pl.DeviceIdType.MESH


def last_source(me, n):
    return jnp.where(2 * me < n, n // 2, n // 2 - 1)


def unit_rows(block):
    return 2 * block + -(-block // (HD * TILE)) * TILE


def kernel(
    n, seqs, chunks, x_hbm, gain_hbm, wk_hbm, wv_hbm, off_hbm, bias_hbm, q_hbm,
    land, off_out, stick, mix_out,
    x_buf, scaled, row_scale, weights, sends, gain_buf, bias_buf, off_in, off_tiles, q_buf,
    x_sem, w_sem, small_sem, land_sem,
):
    total, width = x_buf.shape
    block = total // seqs
    length = n * block
    unit = unit_rows(block)
    me = lax.axis_index("sp")
    order = range(1, n)
    lower = 2 * me < n
    near = jnp.where(lower, me, n - 1 - me)

    def peer(i):
        if i == 0:
            return me
        far = jnp.where(i <= n - 1 - near, n - i, n - 1 - i)
        return jnp.where(lower, far, n - 1 - far)

    def head_of(i):
        return lax.rem(peer(i), KVH)

    gain_copy = pltpu.make_async_copy(gain_hbm, gain_buf, small_sem.at[0])
    x_copies = []
    for c, (start, rows) in enumerate(chunks):
        part = pl.ds(start, rows)
        x_copies.append(pltpu.make_async_copy(x_hbm.at[part], x_buf.at[part], x_sem.at[c]))
    w_copies = []
    for j in range(KVH):
        columns = pl.ds(pl.multiple_of(head_of((j + 1) % n) * HD, HD), HD)
        for kind, w_hbm in enumerate((wk_hbm, wv_hbm)):
            w_copies.append(pltpu.make_async_copy(
                w_hbm.at[:, columns],
                weights.at[j, :, pl.ds(kind * HD, HD)],
                w_sem.at[0 if j else kind],
            ))
    off_copy = pltpu.make_async_copy(off_hbm, off_in, small_sem.at[1])
    q_copy = pltpu.make_async_copy(q_hbm, q_buf, small_sem.at[0])
    bias_copy = pltpu.make_async_copy(bias_hbm, bias_buf, x_sem.at[1])
    gain_copy.start()
    x_copies[0].start()
    w_copies[0].start()
    w_copies[1].start()
    for copy in x_copies[1:]:
        copy.start()
    off_copy.start()

    barrier = pltpu.get_barrier_semaphore()
    for d in order:
        pl.semaphore_signal(
            barrier, inc=1, device_id={"sp": lax.rem(me + d, n)}, device_id_type=MESH
        )

    gain_copy.wait()
    gain = gain_buf[...]

    def prepare(c):
        start, count = chunks[c]
        x_copies[c].wait()

        def step(i, _):
            rows = pl.ds(pl.multiple_of(start + i * STEP, STEP), STEP)
            x = x_buf[rows, :].astype(jnp.float32)
            scaled[rows, :] = (x * gain).astype(jnp.bfloat16)
            scale = lax.rsqrt(jnp.mean(x * x, axis=-1, keepdims=True) + EPSILON)
            row_scale[rows, :] = jnp.broadcast_to(scale, (STEP, HD))
            return 0

        lax.fori_loop(0, count // STEP, step, 0, unroll=4)

    def later_loads():
        for copy in w_copies[2:]:
            copy.start()
        q_copy.start()

    def wait_weights(i):
        if i == 2 % n:
            part = weights.at[pl.ds(1, KVH - 1)]
            pltpu.make_async_copy(part, part, w_sem.at[0]).wait()

    def slot(i):
        if n == KVH:
            return (i - 1) % n
        first = head_of(1)
        down = lax.rem(first - head_of(i) + KVH, KVH)
        return jnp.where(lower, down, lax.rem(KVH - down, KVH))

    def project(i, start, count, columns):
        base = lax.div(peer(i), KVH) * block if seqs > 1 else 0
        rows = pl.ds(pl.multiple_of(base + start, STEP) if seqs > 1 else start, count)
        product = jnp.dot(
            scaled[rows, :], weights[slot(i), :, columns], preferred_element_type=jnp.float32
        )
        scale = row_scale[rows, :]
        return [
            (product[:, c:c + HD] * scale).astype(jnp.bfloat16)
            for c in range(0, product.shape[1], HD)
        ]

    def prepare_and_project(start, count, columns):
        rows = pl.ds(start, count)
        product = jnp.zeros((count, columns.size), jnp.float32)
        squares = jnp.zeros((count, HD), jnp.float32)
        for k in range(0, width, DEPTH):
            part = pl.ds(k, DEPTH)
            x = x_buf[rows, part].astype(jnp.float32)
            y = (x * gain[:, k:k + DEPTH]).astype(jnp.bfloat16)
            scaled[rows, part] = y
            for c in range(0, DEPTH, HD):
                squares = squares + x[:, c:c + HD] * x[:, c:c + HD]
            product = product + jnp.dot(
                y, weights[slot(1), part, columns], preferred_element_type=jnp.float32
            )
        scale = lax.rsqrt(jnp.sum(squares, axis=-1, keepdims=True) / width + EPSILON)
        scale = jnp.broadcast_to(scale, (count, HD))
        row_scale[rows, :] = scale
        return [
            (product[:, c:c + HD] * scale).astype(jnp.bfloat16)
            for c in range(0, columns.size, HD)
        ]

    def remote(src, dst, landed, target):
        return pltpu.make_async_remote_copy(
            src_ref=src, dst_ref=dst, send_sem=x_sem.at[0], recv_sem=landed,
            device_id={"sp": target}, device_id_type=MESH,
        )

    key_part, value_part = pl.ds(0, block), pl.ds(block, block)
    off_part = pl.ds(2 * block, unit - 2 * block)

    def copy_out(i, part, is_value=False):
        is_last = me == last_source(peer(i), n)
        sem = land_sem.at[jnp.where(is_last, 2 if is_value else 1, 0)]
        remote(sends.at[i - 1, part], land.at[me, part], sem, peer(i)).start()

    def lay_offsets():
        off_copy.wait()
        for s in range(seqs):
            values = off_in[s].astype(jnp.float32)
            for h in range(KVH):
                rows = [values[h:h + 1, c:c + HD] for c in range(0, block, HD)]
                blank = jnp.zeros((unit - 2 * block - len(rows), HD), jnp.float32)
                tile = jnp.concatenate(rows + [blank], axis=0)
                off_tiles[s * KVH + h] = tile.astype(jnp.bfloat16)
        for i in order:
            sends[i - 1, off_part] = off_tiles[peer(i)]
        land[me, off_part] = off_tiles[me]

    def greet():
        pl.semaphore_wait(barrier, n - 1)
        for i in order:
            copy_out(i, off_part)

    both = pl.ds(0, 2 * HD)
    lay_offsets()
    if seqs == 1:
        for c, (start, count) in enumerate(chunks):
            x_copies[c].wait()
            keys, values = pl.ds(start, count), pl.ds(block + start, count)
            if c == 0:
                greet()
                w_copies[0].wait()
                sends[0, keys], = prepare_and_project(start, count, pl.ds(0, HD))
                copy_out(1, keys)
                w_copies[1].wait()
                later_loads()
                sends[0, values], = project(1, start, count, pl.ds(HD, HD))
            else:
                sends[0, keys], sends[0, values] = prepare_and_project(start, count, both)
                copy_out(1, keys)
            copy_out(1, values, True)
    else:
        for c in range(len(chunks)):
            prepare(c)
        w_copies[0].wait()
        w_copies[1].wait()
        later_loads()
        sends[0, key_part], sends[0, value_part] = project(1, 0, block, both)
        greet()
        copy_out(1, key_part)
        copy_out(1, value_part, True)
    bias_copy.start()
    for i in order[1:]:
        wait_weights(i)
        sends[i - 1, key_part], sends[i - 1, value_part] = project(i, 0, block, both)
        if i > n // 2:
            copy_out(i, pl.ds(0, 2 * block))
        else:
            copy_out(i, key_part)
            copy_out(i, value_part, True)
    wait_weights(0)
    land[me, key_part], land[me, value_part] = project(0, 0, block, both)

    q_copy.wait()
    q_all = q_buf[0].astype(jnp.float32)
    q_rows = jnp.concatenate([q_all[:, g * HD:(g + 1) * HD] for g in range(GROUP)] * 2, axis=0)
    q_rows = q_rows.astype(jnp.bfloat16)
    bias_copy.wait()
    row_id = lax.broadcasted_iota(jnp.int32, (2 * GROUP, H), 0)
    lane_id = lax.broadcasted_iota(jnp.int32, (2 * GROUP, H), 1)
    chosen = lane_id == lax.rem(me, KVH) * GROUP + lax.rem(row_id, GROUP)
    bias = jnp.sum(jnp.where(chosen, bias_buf[...], 0.0), axis=1, keepdims=True)

    def arrived(part, sem):
        remote(part, part, sem, peer(1)).wait_recv()

    if n > 2:
        arrived(land.at[pl.ds(0, n - 2)], land_sem.at[0])
    arrived(land.at[0, pl.ds(block, unit - block)], land_sem.at[1])
    off_rows = []
    scores = []
    for source in range(n):
        tile = land[source, off_part].astype(jnp.float32)
        off_rows += [tile[c:c + 1] for c in range(block // HD)]
        scores.append(lax.dot_general(
            q_rows, land[source, key_part], (((1,), (1,)), ((), ())),
            preferred_element_type=jnp.float32,
        ))
    off_row = jnp.concatenate(off_rows, axis=1)
    off_out[0] = off_row.astype(jnp.bfloat16)
    scores = jnp.concatenate(scores, axis=1) / math.sqrt(HD) + bias + off_row
    tail = jnp.log1p(jnp.exp(-jnp.abs(scores)))
    spread = jnp.maximum(scores, 0.0) + tail
    log_sig = jnp.minimum(scores, 0.0) - tail
    pieces = length // HD
    cut = [spread[:, c * HD:(c + 1) * HD] for c in range(pieces)]
    stacked = jnp.concatenate(cut, axis=0)
    after = (
        lax.broadcasted_iota(jnp.int32, (HD, HD), 0) > lax.broadcasted_iota(jnp.int32, (HD, HD), 1)
    ).astype(jnp.float32)
    inner = jnp.dot(
        stacked, after, preferred_element_type=jnp.float32, precision=lax.Precision.HIGHEST
    )
    sums = jnp.sum(stacked, axis=1, keepdims=True)
    carried = jnp.zeros((2 * GROUP, 1), jnp.float32)
    for c in reversed(range(pieces)):
        rows = slice(c * 2 * GROUP, (c + 1) * 2 * GROUP)
        beyond = inner[rows] + carried
        stick[:, c * HD:(c + 1) * HD] = jnp.exp(log_sig[:, c * HD:(c + 1) * HD] - beyond)
        carried = carried + sums[rows]

    mixture = jnp.zeros((2 * GROUP, HD), jnp.float32)
    for j in range(n - 1):
        source = lax.rem(last_source(me, n) + 1 + j, n)
        mixture = mixture + read_block(stick, land, source, block)
    mix_out[...] = mixture
    remote(sends, sends, land_sem.at[0], peer(1)).wait_send()
    arrived(land.at[0, value_part], land_sem.at[2])


def read_block(stick, land, source, block):
    part = pl.ds(pl.multiple_of(source * block, block), block)
    return jnp.dot(
        stick[:, part].astype(jnp.bfloat16), land[source, pl.ds(block, block)],
        preferred_element_type=jnp.float32,
    )


def finish(n, land, off_in, stick, mix_in, k_out, v_out, off_out, read_out, read_buf, sem):
    block = k_out.shape[2] // n
    for source in range(n):
        there = pl.ds(source * block, block)
        for kind, cache in enumerate((k_out, v_out)):
            pltpu.make_async_copy(
                land.at[source, pl.ds(kind * block, block)], cache.at[0, 0, there], sem.at[kind]
            ).start()
    off_copy = pltpu.make_async_copy(off_in, off_out, sem.at[2])
    off_copy.start()
    mixture = mix_in[...] + read_block(stick, land, last_source(lax.axis_index("sp"), n), block)
    scale = lax.rsqrt(jnp.mean(mixture * mixture, axis=-1, keepdims=True) + EPSILON)
    read = mixture * scale
    read_buf[0] = jnp.concatenate([read[g:g + 1] for g in range(GROUP)], axis=1).astype(jnp.bfloat16)
    read_copy = pltpu.make_async_copy(read_buf, read_out, sem.at[3])
    read_copy.start()
    for kind, cache in enumerate((k_out, v_out)):
        pltpu.make_async_copy(cache, cache, sem.at[kind]).wait()
    off_copy.wait()
    read_copy.wait()


def chunks_of(seqs, block):
    return tuple((r, ROWS) for r in range(0, seqs * block, ROWS))


def shards(layer_input, input_gain, key_weight, value_weight, stick_offsets, head_bias, queries):
    seqs, block, width = layer_input.shape
    n = lax.axis_size("sp")
    length = n * block
    total = seqs * block
    unit = unit_rows(block)
    hbm = pl.BlockSpec(memory_space=pltpu.HBM)
    vmem = pl.BlockSpec(memory_space=pltpu.VMEM)
    group_width = queries.shape[-1]
    chunks = chunks_of(seqs, block)
    cache = ((1, 1, length, HD), jnp.bfloat16)
    offsets = ((1, 1, length), jnp.bfloat16)
    read = ((1, 1, group_width), jnp.bfloat16)
    held_outs = (
        ((n, unit, HD), jnp.bfloat16),
        offsets,
        ((2 * GROUP, length), jnp.float32),
        ((2 * GROUP, HD), jnp.float32),
    )
    held = pl.pallas_call(
        functools.partial(kernel, n, seqs, chunks),
        out_shape=tuple(pltpu.VMEM(*out) for out in held_outs),
        in_specs=[hbm] * 7,
        out_specs=(vmem,) * len(held_outs),
        scratch_shapes=[
            pltpu.VMEM((total, width), jnp.bfloat16),
            pltpu.VMEM((total, width), jnp.bfloat16),
            pltpu.VMEM((total, HD), jnp.float32),
            pltpu.VMEM((KVH, width, 2 * HD), jnp.bfloat16),
            pltpu.VMEM((n - 1, unit, HD), jnp.bfloat16),
            pltpu.VMEM((1, width), jnp.float32),
            pltpu.VMEM((1, H), jnp.float32),
            pltpu.VMEM((seqs, KVH, block), jnp.bfloat16),
            pltpu.VMEM((n, unit - 2 * block, HD), jnp.bfloat16),
            pltpu.VMEM((1, 1, group_width), jnp.bfloat16),
            pltpu.SemaphoreType.DMA((len(chunks),)),
            pltpu.SemaphoreType.DMA((2,)),
            pltpu.SemaphoreType.DMA((2,)),
            pltpu.SemaphoreType.DMA((3,)),
        ],
        compiler_params=pltpu.CompilerParams(
            collective_id=0, has_side_effects=True, vmem_limit_bytes=VMEM_BYTES - 4 * length * HD - SPARE_BYTES
        ),
    )(
        layer_input.reshape(total, width),
        input_gain.reshape(1, width),
        key_weight,
        value_weight,
        jnp.transpose(stick_offsets, (1, 0, 2)),
        head_bias.reshape(1, H),
        queries,
    )
    outs = (cache, cache, offsets, read)
    return pl.pallas_call(
        functools.partial(finish, n),
        out_shape=tuple(jax.ShapeDtypeStruct(*out) for out in outs),
        in_specs=[vmem] * len(held_outs),
        out_specs=(hbm,) * len(outs),
        scratch_shapes=[
            pltpu.VMEM(*read),
            pltpu.SemaphoreType.DMA((len(outs),)),
        ],
        compiler_params=pltpu.CompilerParams(vmem_limit_bytes=WRITE_BYTES),
    )(*held)


def solution(mesh):
    placed = (
        P(("grp", "tp"), "sp", None),
        P(),
        P(),
        P(),
        P(None, ("grp", "tp"), "sp"),
        P(),
        P(("grp", "tp"), "sp", None),
    )
    return jax.shard_map(
        shards,
        mesh=mesh,
        in_specs=placed,
        out_specs=(
            P(("grp", "tp"), "sp", None, None),
            P(("grp", "tp"), "sp", None, None),
            P(("grp", "tp"), "sp", None),
            P(("grp", "tp"), "sp", None),
        ),
        check_vma=False,
    )
```

```python
import functools
import math

import jax
import jax.numpy as jnp
from jax import lax
from jax.experimental import pallas as pl
from jax.experimental.pallas import tpu as pltpu
from jax.sharding import PartitionSpec as P

H = 16
KVH = 4
HD = 128
GROUP = H // KVH
EPSILON = 1e-06
ROWS = 128
STEP = 16
TILE = 8
DEPTH = 256
VMEM_BYTES = 67043328
SPARE_BYTES = 524288
WRITE_BYTES = 1048576
MESH = pl.DeviceIdType.MESH


def last_source(me, n):
    return jnp.where(2 * me < n, n // 2, n // 2 - 1)


def unit_rows(block):
    return 2 * block + -(-block // (HD * TILE)) * TILE


def kernel(
    n, seqs, chunks, x_hbm, gain_hbm, wk_hbm, wv_hbm, off_hbm, bias_hbm, q_hbm,
    land, off_out, stick, mix_out,
    x_buf, scaled, row_scale, weights, sends, gain_buf, bias_buf, off_in, off_tiles, q_buf,
    x_sem, w_sem, small_sem, land_sem,
):
    total, width = x_buf.shape
    block = total // seqs
    length = n * block
    unit = unit_rows(block)
    me = lax.axis_index("sp")
    order = range(1, n)
    lower = 2 * me < n
    near = jnp.where(lower, me, n - 1 - me)

    def peer(i):
        if i == 0:
            return me
        if i == 1:
            return jnp.where(lower, n - 1, 0)
        far = jnp.where(i <= n - 1 - near, n - i, n - 1 - i)
        return jnp.where(lower, far, n - 1 - far)

    def head_of(i):
        return lax.rem(peer(i), KVH)

    gain_copy = pltpu.make_async_copy(gain_hbm, gain_buf, small_sem.at[0])
    x_copies = []
    for c, (start, rows) in enumerate(chunks):
        part = pl.ds(start, rows)
        x_copies.append(pltpu.make_async_copy(x_hbm.at[part], x_buf.at[part], x_sem.at[c]))
    w_copies = []
    for j in range(KVH):
        columns = pl.ds(pl.multiple_of(head_of((j + 1) % n) * HD, HD), HD)
        for kind, w_hbm in enumerate((wk_hbm, wv_hbm)):
            w_copies.append(pltpu.make_async_copy(
                w_hbm.at[:, columns],
                weights.at[j, :, pl.ds(kind * HD, HD)],
                w_sem.at[0 if j else kind],
            ))
    off_copy = pltpu.make_async_copy(off_hbm, off_in, small_sem.at[1])
    q_copy = pltpu.make_async_copy(q_hbm, q_buf, small_sem.at[0])
    bias_copy = pltpu.make_async_copy(bias_hbm, bias_buf, x_sem.at[1])
    gain_copy.start()
    x_copies[0].start()
    w_copies[0].start()
    w_copies[1].start()
    for copy in x_copies[1:]:
        copy.start()
    off_copy.start()

    barrier = pltpu.get_barrier_semaphore()
    for d in order:
        pl.semaphore_signal(
            barrier, inc=1, device_id={"sp": lax.rem(me + d, n)}, device_id_type=MESH
        )

    gain_copy.wait()
    gain = gain_buf[...]

    def prepare(c):
        start, count = chunks[c]
        x_copies[c].wait()

        def step(i, _):
            rows = pl.ds(pl.multiple_of(start + i * STEP, STEP), STEP)
            x = x_buf[rows, :].astype(jnp.float32)
            scaled[rows, :] = (x * gain).astype(jnp.bfloat16)
            scale = lax.rsqrt(jnp.mean(x * x, axis=-1, keepdims=True) + EPSILON)
            row_scale[rows, :] = jnp.broadcast_to(scale, (STEP, HD))
            return 0

        lax.fori_loop(0, count // STEP, step, 0, unroll=4)

    def later_loads():
        for copy in w_copies[2:]:
            copy.start()
        q_copy.start()

    def wait_weights(i):
        if i == 2 % n:
            part = weights.at[pl.ds(1, KVH - 1)]
            pltpu.make_async_copy(part, part, w_sem.at[0]).wait()

    def slot(i):
        if n == KVH:
            return (i - 1) % n
        first = head_of(1)
        down = lax.rem(first - head_of(i) + KVH, KVH)
        return jnp.where(lower, down, lax.rem(KVH - down, KVH))

    def project(i, start, count, columns):
        base = lax.div(peer(i), KVH) * block if seqs > 1 else 0
        rows = pl.ds(pl.multiple_of(base + start, STEP) if seqs > 1 else start, count)
        product = jnp.dot(
            scaled[rows, :], weights[slot(i), :, columns], preferred_element_type=jnp.float32
        )
        scale = row_scale[rows, :]
        return [
            (product[:, c:c + HD] * scale).astype(jnp.bfloat16)
            for c in range(0, product.shape[1], HD)
        ]

    def prepare_and_project(start, count, columns):
        rows = pl.ds(start, count)
        product = jnp.zeros((count, columns.size), jnp.float32)
        squares = jnp.zeros((count, HD), jnp.float32)
        for k in range(0, width, DEPTH):
            part = pl.ds(k, DEPTH)
            x = x_buf[rows, part].astype(jnp.float32)
            y = (x * gain[:, k:k + DEPTH]).astype(jnp.bfloat16)
            scaled[rows, part] = y
            for c in range(0, DEPTH, HD):
                squares = squares + x[:, c:c + HD] * x[:, c:c + HD]
            product = product + jnp.dot(
                y, weights[slot(1), part, columns], preferred_element_type=jnp.float32
            )
        scale = lax.rsqrt(jnp.sum(squares, axis=-1, keepdims=True) / width + EPSILON)
        scale = jnp.broadcast_to(scale, (count, HD))
        row_scale[rows, :] = scale
        return [
            (product[:, c:c + HD] * scale).astype(jnp.bfloat16)
            for c in range(0, columns.size, HD)
        ]

    def remote(src, dst, landed, target):
        return pltpu.make_async_remote_copy(
            src_ref=src, dst_ref=dst, send_sem=x_sem.at[0], recv_sem=landed,
            device_id={"sp": target}, device_id_type=MESH,
        )

    key_part, value_part = pl.ds(0, block), pl.ds(block, block)
    off_part = pl.ds(2 * block, unit - 2 * block)

    def copy_out(i, part, is_value=False):
        is_last = me == last_source(peer(i), n)
        sem = land_sem.at[jnp.where(is_last, 2 if is_value else 1, 0)]
        remote(sends.at[i - 1, part], land.at[me, part], sem, peer(i)).start()

    def lay_offsets():
        off_copy.wait()
        for s in range(seqs):
            values = off_in[s].astype(jnp.float32)
            for h in range(KVH):
                rows = [values[h:h + 1, c:c + HD] for c in range(0, block, HD)]
                blank = jnp.zeros((unit - 2 * block - len(rows), HD), jnp.float32)
                tile = jnp.concatenate(rows + [blank], axis=0)
                off_tiles[s * KVH + h] = tile.astype(jnp.bfloat16)
        for i in order:
            sends[i - 1, off_part] = off_tiles[peer(i)]
        land[me, off_part] = off_tiles[me]

    def greet():
        pl.semaphore_wait(barrier, n - 1)
        for i in order:
            copy_out(i, off_part)

    both = pl.ds(0, 2 * HD)
    if seqs > 1:
        lay_offsets()
    if seqs == 1:
        for c, (start, count) in enumerate(chunks):
            x_copies[c].wait()
            if c == len(chunks) - 1:
                later_loads()
            keys, values = pl.ds(start, count), pl.ds(block + start, count)
            if c == 0:
                w_copies[0].wait()
                sends[0, keys], = prepare_and_project(start, count, pl.ds(0, HD))
                pl.semaphore_wait(barrier, n - 1)
                copy_out(1, keys)
                lay_offsets()
                for i in order:
                    copy_out(i, off_part)
                w_copies[1].wait()
                sends[0, values], = project(1, start, count, pl.ds(HD, HD))
            else:
                sends[0, keys], sends[0, values] = prepare_and_project(start, count, both)
                copy_out(1, keys)
            copy_out(1, values, True)
    else:
        for c in range(len(chunks)):
            prepare(c)
        w_copies[0].wait()
        w_copies[1].wait()
        later_loads()
        sends[0, key_part], sends[0, value_part] = project(1, 0, block, both)
        greet()
        copy_out(1, key_part)
        copy_out(1, value_part, True)
    bias_copy.start()
    for i in order[1:]:
        wait_weights(i)
        sends[i - 1, key_part], sends[i - 1, value_part] = project(i, 0, block, both)
        if i > n // 2:
            copy_out(i, pl.ds(0, 2 * block))
        else:
            copy_out(i, key_part)
            copy_out(i, value_part, True)
    wait_weights(0)
    land[me, key_part], land[me, value_part] = project(0, 0, block, both)

    q_copy.wait()
    q_all = q_buf[0].astype(jnp.float32)
    q_rows = jnp.concatenate([q_all[:, g * HD:(g + 1) * HD] for g in range(GROUP)] * 2, axis=0)
    q_rows = q_rows.astype(jnp.bfloat16)
    bias_copy.wait()
    row_id = lax.broadcasted_iota(jnp.int32, (2 * GROUP, H), 0)
    lane_id = lax.broadcasted_iota(jnp.int32, (2 * GROUP, H), 1)
    chosen = lane_id == lax.rem(me, KVH) * GROUP + lax.rem(row_id, GROUP)
    bias = jnp.sum(jnp.where(chosen, bias_buf[...], 0.0), axis=1, keepdims=True)

    def arrived(part, sem):
        remote(part, part, sem, peer(1)).wait_recv()

    if n > 2:
        arrived(land.at[pl.ds(0, n - 2)], land_sem.at[0])
    arrived(land.at[0, pl.ds(block, unit - block)], land_sem.at[1])
    off_rows = []
    scores = []
    for source in range(n):
        tile = land[source, off_part].astype(jnp.float32)
        off_rows += [tile[c:c + 1] for c in range(block // HD)]
        scores.append(lax.dot_general(
            q_rows, land[source, key_part], (((1,), (1,)), ((), ())),
            preferred_element_type=jnp.float32,
        ))
    off_row = jnp.concatenate(off_rows, axis=1)
    off_out[0] = off_row.astype(jnp.bfloat16)
    scores = jnp.concatenate(scores, axis=1) / math.sqrt(HD) + bias + off_row
    tail = jnp.log1p(jnp.exp(-jnp.abs(scores)))
    spread = jnp.maximum(scores, 0.0) + tail
    log_sig = jnp.minimum(scores, 0.0) - tail
    pieces = length // HD
    cut = [spread[:, c * HD:(c + 1) * HD] for c in range(pieces)]
    stacked = jnp.concatenate(cut, axis=0)
    after = (
        lax.broadcasted_iota(jnp.int32, (HD, HD), 0) > lax.broadcasted_iota(jnp.int32, (HD, HD), 1)
    ).astype(jnp.float32)
    inner = jnp.dot(
        stacked, after, preferred_element_type=jnp.float32, precision=lax.Precision.HIGHEST
    )
    sums = jnp.sum(stacked, axis=1, keepdims=True)
    carried = jnp.zeros((2 * GROUP, 1), jnp.float32)
    for c in reversed(range(pieces)):
        rows = slice(c * 2 * GROUP, (c + 1) * 2 * GROUP)
        beyond = inner[rows] + carried
        stick[:, c * HD:(c + 1) * HD] = jnp.exp(log_sig[:, c * HD:(c + 1) * HD] - beyond)
        carried = carried + sums[rows]

    mixture = jnp.zeros((2 * GROUP, HD), jnp.float32)
    for j in range(n - 1):
        source = lax.rem(last_source(me, n) + 1 + j, n)
        mixture = mixture + read_block(stick, land, source, block)
    mix_out[...] = mixture
    remote(sends, sends, land_sem.at[0], peer(1)).wait_send()
    arrived(land.at[0, value_part], land_sem.at[2])


def read_block(stick, land, source, block):
    part = pl.ds(pl.multiple_of(source * block, block), block)
    return jnp.dot(
        stick[:, part].astype(jnp.bfloat16), land[source, pl.ds(block, block)],
        preferred_element_type=jnp.float32,
    )


def finish(n, land, off_in, stick, mix_in, k_out, v_out, off_out, read_out, read_buf, sem):
    block = k_out.shape[2] // n
    for source in range(n):
        there = pl.ds(source * block, block)
        for kind, cache in enumerate((k_out, v_out)):
            pltpu.make_async_copy(
                land.at[source, pl.ds(kind * block, block)], cache.at[0, 0, there], sem.at[kind]
            ).start()
    off_copy = pltpu.make_async_copy(off_in, off_out, sem.at[2])
    off_copy.start()
    mixture = mix_in[...] + read_block(stick, land, last_source(lax.axis_index("sp"), n), block)
    scale = lax.rsqrt(jnp.mean(mixture * mixture, axis=-1, keepdims=True) + EPSILON)
    read = mixture * scale
    read_buf[0] = jnp.concatenate([read[g:g + 1] for g in range(GROUP)], axis=1).astype(jnp.bfloat16)
    read_copy = pltpu.make_async_copy(read_buf, read_out, sem.at[3])
    read_copy.start()
    for kind, cache in enumerate((k_out, v_out)):
        pltpu.make_async_copy(cache, cache, sem.at[kind]).wait()
    off_copy.wait()
    read_copy.wait()


def chunks_of(seqs, block):
    return tuple((r, ROWS) for r in range(0, seqs * block, ROWS))


def shards(layer_input, input_gain, key_weight, value_weight, stick_offsets, head_bias, queries):
    seqs, block, width = layer_input.shape
    n = lax.axis_size("sp")
    length = n * block
    total = seqs * block
    unit = unit_rows(block)
    hbm = pl.BlockSpec(memory_space=pltpu.HBM)
    vmem = pl.BlockSpec(memory_space=pltpu.VMEM)
    group_width = queries.shape[-1]
    chunks = chunks_of(seqs, block)
    cache = ((1, 1, length, HD), jnp.bfloat16)
    offsets = ((1, 1, length), jnp.bfloat16)
    read = ((1, 1, group_width), jnp.bfloat16)
    held_outs = (
        ((n, unit, HD), jnp.bfloat16),
        offsets,
        ((2 * GROUP, length), jnp.float32),
        ((2 * GROUP, HD), jnp.float32),
    )
    held = pl.pallas_call(
        functools.partial(kernel, n, seqs, chunks),
        out_shape=tuple(pltpu.VMEM(*out) for out in held_outs),
        in_specs=[hbm] * 7,
        out_specs=(vmem,) * len(held_outs),
        scratch_shapes=[
            pltpu.VMEM((total, width), jnp.bfloat16),
            pltpu.VMEM((total, width), jnp.bfloat16),
            pltpu.VMEM((total, HD), jnp.float32),
            pltpu.VMEM((KVH, width, 2 * HD), jnp.bfloat16),
            pltpu.VMEM((n - 1, unit, HD), jnp.bfloat16),
            pltpu.VMEM((1, width), jnp.float32),
            pltpu.VMEM((1, H), jnp.float32),
            pltpu.VMEM((seqs, KVH, block), jnp.bfloat16),
            pltpu.VMEM((n, unit - 2 * block, HD), jnp.bfloat16),
            pltpu.VMEM((1, 1, group_width), jnp.bfloat16),
            pltpu.SemaphoreType.DMA((len(chunks),)),
            pltpu.SemaphoreType.DMA((2,)),
            pltpu.SemaphoreType.DMA((2,)),
            pltpu.SemaphoreType.DMA((3,)),
        ],
        compiler_params=pltpu.CompilerParams(
            collective_id=0, has_side_effects=True, vmem_limit_bytes=VMEM_BYTES - 4 * length * HD - SPARE_BYTES
        ),
    )(
        layer_input.reshape(total, width),
        input_gain.reshape(1, width),
        key_weight,
        value_weight,
        jnp.transpose(stick_offsets, (1, 0, 2)),
        head_bias.reshape(1, H),
        queries,
    )
    outs = (cache, cache, offsets, read)
    return pl.pallas_call(
        functools.partial(finish, n),
        out_shape=tuple(jax.ShapeDtypeStruct(*out) for out in outs),
        in_specs=[vmem] * len(held_outs),
        out_specs=(hbm,) * len(outs),
        scratch_shapes=[
            pltpu.VMEM(*read),
            pltpu.SemaphoreType.DMA((len(outs),)),
        ],
        compiler_params=pltpu.CompilerParams(vmem_limit_bytes=WRITE_BYTES),
    )(*held)


def solution(mesh):
    placed = (
        P(("grp", "tp"), "sp", None),
        P(),
        P(),
        P(),
        P(None, ("grp", "tp"), "sp"),
        P(),
        P(("grp", "tp"), "sp", None),
    )
    return jax.shard_map(
        shards,
        mesh=mesh,
        in_specs=placed,
        out_specs=(
            P(("grp", "tp"), "sp", None, None),
            P(("grp", "tp"), "sp", None, None),
            P(("grp", "tp"), "sp", None),
            P(("grp", "tp"), "sp", None),
        ),
        check_vma=False,
    )
```

```python
import functools
import math

import jax
import jax.numpy as jnp
from jax import lax
from jax.experimental import pallas as pl
from jax.experimental.pallas import tpu as pltpu
from jax.sharding import PartitionSpec as P

H = 16
KVH = 4
HD = 128
GROUP = H // KVH
EPSILON = 1e-06
ROWS = 128
STEP = 16
TILE = 8
DEPTH = 256
VMEM_BYTES = 67043328
SPARE_BYTES = 524288
WRITE_BYTES = 1048576
MESH = pl.DeviceIdType.MESH


def last_source(me, n):
    return jnp.where(2 * me < n, n // 2, n // 2 - 1)


def unit_rows(block):
    return 2 * block + -(-block // (HD * TILE)) * TILE


def kernel(
    n, seqs, chunks, x_hbm, gain_hbm, wk_hbm, wv_hbm, off_hbm, bias_hbm, q_hbm,
    land, off_out, stick, mix_out,
    x_buf, scaled, row_scale, weights, sends, gain_buf, bias_buf, off_in, off_tiles, q_buf,
    x_sem, w_sem, small_sem, land_sem,
):
    total, width = x_buf.shape
    block = total // seqs
    length = n * block
    unit = unit_rows(block)
    me = lax.axis_index("sp")
    order = range(1, n)
    lower = 2 * me < n
    near = jnp.where(lower, me, n - 1 - me)

    def peer(i):
        if i == 0:
            return me
        if i == 1:
            return jnp.where(lower, n - 1, 0)
        far = jnp.where(i <= n - 1 - near, n - i, n - 1 - i)
        return jnp.where(lower, far, n - 1 - far)

    def head_of(i):
        return lax.rem(peer(i), KVH)

    gain_copy = pltpu.make_async_copy(gain_hbm, gain_buf, small_sem.at[0])
    x_copies = []
    for c, (start, rows) in enumerate(chunks):
        part = pl.ds(start, rows)
        x_copies.append(pltpu.make_async_copy(x_hbm.at[part], x_buf.at[part], x_sem.at[c]))
    w_copies = []
    for j in range(KVH):
        columns = pl.ds(pl.multiple_of(head_of((j + 1) % n) * HD, HD), HD)
        for kind, w_hbm in enumerate((wk_hbm, wv_hbm)):
            w_copies.append(pltpu.make_async_copy(
                w_hbm.at[:, columns],
                weights.at[j, :, pl.ds(kind * HD, HD)],
                w_sem.at[0 if j else kind],
            ))
    off_copy = pltpu.make_async_copy(off_hbm, off_in, small_sem.at[1])
    q_copy = pltpu.make_async_copy(q_hbm, q_buf, small_sem.at[0])
    bias_copy = pltpu.make_async_copy(bias_hbm, bias_buf, x_sem.at[1])
    gain_copy.start()
    x_copies[0].start()
    w_copies[0].start()
    w_copies[1].start()
    for copy in x_copies[1:]:
        copy.start()
    off_copy.start()

    barrier = pltpu.get_barrier_semaphore()
    for d in order:
        pl.semaphore_signal(
            barrier, inc=1, device_id={"sp": lax.rem(me + d, n)}, device_id_type=MESH
        )

    gain_copy.wait()
    gain = gain_buf[...]

    def prepare(c):
        start, count = chunks[c]
        x_copies[c].wait()

        def step(i, _):
            rows = pl.ds(pl.multiple_of(start + i * STEP, STEP), STEP)
            x = x_buf[rows, :].astype(jnp.float32)
            scaled[rows, :] = (x * gain).astype(jnp.bfloat16)
            scale = lax.rsqrt(jnp.mean(x * x, axis=-1, keepdims=True) + EPSILON)
            row_scale[rows, :] = jnp.broadcast_to(scale, (STEP, HD))
            return 0

        lax.fori_loop(0, count // STEP, step, 0, unroll=4)

    def later_loads():
        for copy in w_copies[2:]:
            copy.start()
        q_copy.start()

    def wait_weights(i):
        if i == 2 % n:
            part = weights.at[pl.ds(1, KVH - 1)]
            pltpu.make_async_copy(part, part, w_sem.at[0]).wait()

    def slot(i):
        if n == KVH:
            return (i - 1) % n
        first = head_of(1)
        down = lax.rem(first - head_of(i) + KVH, KVH)
        return jnp.where(lower, down, lax.rem(KVH - down, KVH))

    def project(i, start, count, columns):
        base = lax.div(peer(i), KVH) * block if seqs > 1 else 0
        rows = pl.ds(pl.multiple_of(base + start, STEP) if seqs > 1 else start, count)
        product = jnp.dot(
            scaled[rows, :], weights[slot(i), :, columns], preferred_element_type=jnp.float32
        )
        scale = row_scale[rows, :]
        return [
            (product[:, c:c + HD] * scale).astype(jnp.bfloat16)
            for c in range(0, product.shape[1], HD)
        ]

    def prepare_and_project(start, count, columns):
        rows = pl.ds(start, count)
        product = jnp.zeros((count, columns.size), jnp.float32)
        squares = jnp.zeros((count, HD), jnp.float32)
        for k in range(0, width, DEPTH):
            part = pl.ds(k, DEPTH)
            x = x_buf[rows, part].astype(jnp.float32)
            y = (x * gain[:, k:k + DEPTH]).astype(jnp.bfloat16)
            scaled[rows, part] = y
            for c in range(0, DEPTH, HD):
                squares = squares + x[:, c:c + HD] * x[:, c:c + HD]
            product = product + jnp.dot(
                y, weights[slot(1), part, columns], preferred_element_type=jnp.float32
            )
        scale = lax.rsqrt(jnp.sum(squares, axis=-1, keepdims=True) / width + EPSILON)
        scale = jnp.broadcast_to(scale, (count, HD))
        row_scale[rows, :] = scale
        return [
            (product[:, c:c + HD] * scale).astype(jnp.bfloat16)
            for c in range(0, columns.size, HD)
        ]

    def remote(src, dst, landed, target):
        return pltpu.make_async_remote_copy(
            src_ref=src, dst_ref=dst, send_sem=x_sem.at[0], recv_sem=landed,
            device_id={"sp": target}, device_id_type=MESH,
        )

    key_part, value_part = pl.ds(0, block), pl.ds(block, block)
    off_part = pl.ds(2 * block, unit - 2 * block)

    def copy_out(i, part, is_value=False):
        is_last = me == last_source(peer(i), n)
        sem = land_sem.at[jnp.where(is_last, 2 if is_value else 1, 0)]
        remote(sends.at[i - 1, part], land.at[me, part], sem, peer(i)).start()

    def lay_offsets():
        off_copy.wait()
        for s in range(seqs):
            values = off_in[s].astype(jnp.float32)
            for h in range(KVH):
                rows = [values[h:h + 1, c:c + HD] for c in range(0, block, HD)]
                blank = jnp.zeros((unit - 2 * block - len(rows), HD), jnp.float32)
                tile = jnp.concatenate(rows + [blank], axis=0)
                off_tiles[s * KVH + h] = tile.astype(jnp.bfloat16)
        for i in order:
            sends[i - 1, off_part] = off_tiles[peer(i)]
        land[me, off_part] = off_tiles[me]

    def greet():
        pl.semaphore_wait(barrier, n - 1)
        for i in order:
            copy_out(i, off_part)

    both = pl.ds(0, 2 * HD)
    if seqs > 1:
        lay_offsets()
    if seqs == 1:
        for c, (start, count) in enumerate(chunks):
            x_copies[c].wait()
            if c == len(chunks) - 1:
                later_loads()
            keys, values = pl.ds(start, count), pl.ds(block + start, count)
            if c == 0:
                w_copies[0].wait()
                sends[0, keys], = prepare_and_project(start, count, pl.ds(0, HD))
                pl.semaphore_wait(barrier, n - 1)
                copy_out(1, keys)
                lay_offsets()
                for i in order:
                    copy_out(i, off_part)
                w_copies[1].wait()
                sends[0, values], = project(1, start, count, pl.ds(HD, HD))
            else:
                sends[0, keys], sends[0, values] = prepare_and_project(start, count, both)
                copy_out(1, keys)
            copy_out(1, values, True)
    else:
        for c in range(len(chunks)):
            prepare(c)
        w_copies[0].wait()
        w_copies[1].wait()
        later_loads()
        sends[0, key_part], sends[0, value_part] = project(1, 0, block, both)
        greet()
        copy_out(1, key_part)
        copy_out(1, value_part, True)
    bias_copy.start()
    for i in order[1:]:
        wait_weights(i)
        sends[i - 1, key_part], sends[i - 1, value_part] = project(i, 0, block, both)
        if i > n // 2:
            copy_out(i, pl.ds(0, 2 * block))
        else:
            copy_out(i, key_part)
            copy_out(i, value_part, True)
    wait_weights(0)
    land[me, key_part], land[me, value_part] = project(0, 0, block, both)

    q_copy.wait()
    q_all = q_buf[0].astype(jnp.float32)
    q_rows = jnp.concatenate([q_all[:, g * HD:(g + 1) * HD] for g in range(GROUP)] * 2, axis=0)
    q_rows = q_rows.astype(jnp.bfloat16)
    bias_copy.wait()
    row_id = lax.broadcasted_iota(jnp.int32, (2 * GROUP, H), 0)
    lane_id = lax.broadcasted_iota(jnp.int32, (2 * GROUP, H), 1)
    chosen = lane_id == lax.rem(me, KVH) * GROUP + lax.rem(row_id, GROUP)
    bias = jnp.sum(jnp.where(chosen, bias_buf[...], 0.0), axis=1, keepdims=True)

    def arrived(part, sem):
        remote(part, part, sem, peer(1)).wait_recv()

    if n > 2:
        arrived(land.at[pl.ds(0, n - 2)], land_sem.at[0])
    arrived(land.at[0, pl.ds(block, unit - block)], land_sem.at[1])
    off_rows = []
    scores = []
    for source in range(n):
        tile = land[source, off_part].astype(jnp.float32)
        off_rows += [tile[c:c + 1] for c in range(block // HD)]
        scores.append(lax.dot_general(
            q_rows, land[source, key_part], (((1,), (1,)), ((), ())),
            preferred_element_type=jnp.float32,
        ))
    off_row = jnp.concatenate(off_rows, axis=1)
    off_out[0] = off_row.astype(jnp.bfloat16)
    scores = jnp.concatenate(scores, axis=1) / math.sqrt(HD) + bias + off_row
    tail = jnp.log1p(jnp.exp(-jnp.abs(scores)))
    spread = jnp.maximum(scores, 0.0) + tail
    log_sig = jnp.minimum(scores, 0.0) - tail
    pieces = length // HD
    cut = [spread[:, c * HD:(c + 1) * HD] for c in range(pieces)]
    stacked = jnp.concatenate(cut, axis=0)
    after = (
        lax.broadcasted_iota(jnp.int32, (HD, HD), 0) > lax.broadcasted_iota(jnp.int32, (HD, HD), 1)
    ).astype(jnp.float32)
    inner = jnp.dot(
        stacked, after, preferred_element_type=jnp.float32, precision=lax.Precision.HIGHEST
    )
    sums = jnp.sum(stacked, axis=1, keepdims=True)
    carried = jnp.zeros((2 * GROUP, 1), jnp.float32)
    for c in reversed(range(pieces)):
        rows = slice(c * 2 * GROUP, (c + 1) * 2 * GROUP)
        beyond = inner[rows] + carried
        stick[:, c * HD:(c + 1) * HD] = jnp.exp(log_sig[:, c * HD:(c + 1) * HD] - beyond)
        carried = carried + sums[rows]

    mixture = jnp.zeros((2 * GROUP, HD), jnp.float32)
    for j in range(n - 1):
        source = lax.rem(last_source(me, n) + 1 + j, n)
        mixture = mixture + read_block(stick, land, source, block)
    mix_out[...] = mixture
    remote(sends, sends, land_sem.at[0], peer(1)).wait_send()
    arrived(land.at[0, value_part], land_sem.at[2])


def read_block(stick, land, source, block):
    part = pl.ds(pl.multiple_of(source * block, block), block)
    return jnp.dot(
        stick[:, part].astype(jnp.bfloat16), land[source, pl.ds(block, block)],
        preferred_element_type=jnp.float32,
    )


def finish(n, land, off_in, stick, mix_in, k_out, v_out, off_out, read_out, read_buf, sem):
    block = k_out.shape[2] // n
    for source in range(n):
        there = pl.ds(source * block, block)
        for kind, cache in enumerate((k_out, v_out)):
            pltpu.make_async_copy(
                land.at[source, pl.ds(kind * block, block)], cache.at[0, 0, there], sem.at[0]
            ).start()
    off_copy = pltpu.make_async_copy(off_in, off_out, sem.at[1])
    off_copy.start()
    mixture = mix_in[...] + read_block(stick, land, last_source(lax.axis_index("sp"), n), block)
    scale = lax.rsqrt(jnp.mean(mixture * mixture, axis=-1, keepdims=True) + EPSILON)
    read = mixture * scale
    read_buf[0] = jnp.concatenate([read[g:g + 1] for g in range(GROUP)], axis=1).astype(jnp.bfloat16)
    read_copy = pltpu.make_async_copy(read_buf, read_out, sem.at[2])
    read_copy.start()
    caches = land.at[:, pl.ds(0, 2 * block)]
    pltpu.make_async_copy(caches, caches, sem.at[0]).wait()
    off_copy.wait()
    read_copy.wait()


def chunks_of(seqs, block):
    return tuple((r, ROWS) for r in range(0, seqs * block, ROWS))


def shards(layer_input, input_gain, key_weight, value_weight, stick_offsets, head_bias, queries):
    seqs, block, width = layer_input.shape
    n = lax.axis_size("sp")
    length = n * block
    total = seqs * block
    unit = unit_rows(block)
    hbm = pl.BlockSpec(memory_space=pltpu.HBM)
    vmem = pl.BlockSpec(memory_space=pltpu.VMEM)
    group_width = queries.shape[-1]
    chunks = chunks_of(seqs, block)
    cache = ((1, 1, length, HD), jnp.bfloat16)
    offsets = ((1, 1, length), jnp.bfloat16)
    read = ((1, 1, group_width), jnp.bfloat16)
    held_outs = (
        ((n, unit, HD), jnp.bfloat16),
        offsets,
        ((2 * GROUP, length), jnp.float32),
        ((2 * GROUP, HD), jnp.float32),
    )
    held = pl.pallas_call(
        functools.partial(kernel, n, seqs, chunks),
        out_shape=tuple(pltpu.VMEM(*out) for out in held_outs),
        in_specs=[hbm] * 7,
        out_specs=(vmem,) * len(held_outs),
        scratch_shapes=[
            pltpu.VMEM((total, width), jnp.bfloat16),
            pltpu.VMEM((total, width), jnp.bfloat16),
            pltpu.VMEM((total, HD), jnp.float32),
            pltpu.VMEM((KVH, width, 2 * HD), jnp.bfloat16),
            pltpu.VMEM((n - 1, unit, HD), jnp.bfloat16),
            pltpu.VMEM((1, width), jnp.float32),
            pltpu.VMEM((1, H), jnp.float32),
            pltpu.VMEM((seqs, KVH, block), jnp.bfloat16),
            pltpu.VMEM((n, unit - 2 * block, HD), jnp.bfloat16),
            pltpu.VMEM((1, 1, group_width), jnp.bfloat16),
            pltpu.SemaphoreType.DMA((len(chunks),)),
            pltpu.SemaphoreType.DMA((2,)),
            pltpu.SemaphoreType.DMA((2,)),
            pltpu.SemaphoreType.DMA((3,)),
        ],
        compiler_params=pltpu.CompilerParams(
            collective_id=0, has_side_effects=True, vmem_limit_bytes=VMEM_BYTES - 4 * length * HD - SPARE_BYTES
        ),
    )(
        layer_input.reshape(total, width),
        input_gain.reshape(1, width),
        key_weight,
        value_weight,
        jnp.transpose(stick_offsets, (1, 0, 2)),
        head_bias.reshape(1, H),
        queries,
    )
    outs = (cache, cache, offsets, read)
    return pl.pallas_call(
        functools.partial(finish, n),
        out_shape=tuple(jax.ShapeDtypeStruct(*out) for out in outs),
        in_specs=[vmem] * len(held_outs),
        out_specs=(hbm,) * len(outs),
        scratch_shapes=[
            pltpu.VMEM(*read),
            pltpu.SemaphoreType.DMA((3,)),
        ],
        compiler_params=pltpu.CompilerParams(vmem_limit_bytes=WRITE_BYTES),
    )(*held)


def solution(mesh):
    placed = (
        P(("grp", "tp"), "sp", None),
        P(),
        P(),
        P(),
        P(None, ("grp", "tp"), "sp"),
        P(),
        P(("grp", "tp"), "sp", None),
    )
    return jax.shard_map(
        shards,
        mesh=mesh,
        in_specs=placed,
        out_specs=(
            P(("grp", "tp"), "sp", None, None),
            P(("grp", "tp"), "sp", None, None),
            P(("grp", "tp"), "sp", None),
            P(("grp", "tp"), "sp", None),
        ),
        check_vma=False,
    )
```

```python
import functools
import math

import jax
import jax.numpy as jnp
from jax import lax
from jax.experimental import pallas as pl
from jax.experimental.pallas import tpu as pltpu
from jax.sharding import PartitionSpec as P

H = 16
KVH = 4
HD = 128
GROUP = H // KVH
EPSILON = 1e-06
ROWS = 128
STEP = 16
TILE = 8
DEPTH = 256
VMEM_BYTES = 67043328
SPARE_BYTES = 524288
WRITE_BYTES = 1048576
MESH = pl.DeviceIdType.MESH


def last_source(me, n):
    return jnp.where(2 * me < n, n // 2, n // 2 - 1)


def unit_rows(block):
    return 2 * block + -(-block // (HD * TILE)) * TILE


def kernel(
    n, seqs, chunks, x_hbm, gain_hbm, wk_hbm, wv_hbm, off_hbm, bias_hbm, q_hbm,
    land, off_out, stick, mix_out,
    x_buf, normed, weights, sends, gain_buf, bias_buf, off_in, off_tiles, q_buf,
    x_sem, w_sem, small_sem, land_sem,
):
    total, width = x_buf.shape
    block = total // seqs
    length = n * block
    unit = unit_rows(block)
    me = lax.axis_index("sp")
    order = range(1, n)
    lower = 2 * me < n
    near = jnp.where(lower, me, n - 1 - me)

    def peer(i):
        if i == 0:
            return me
        if i == 1:
            return jnp.where(lower, n - 1, 0)
        far = jnp.where(i <= n - 1 - near, n - i, n - 1 - i)
        return jnp.where(lower, far, n - 1 - far)

    def head_of(i):
        return lax.rem(peer(i), KVH)

    gain_copy = pltpu.make_async_copy(gain_hbm, gain_buf, small_sem.at[0])
    x_copies = []
    for c, (start, rows) in enumerate(chunks):
        part = pl.ds(start, rows)
        x_copies.append(pltpu.make_async_copy(x_hbm.at[part], x_buf.at[part], x_sem.at[c]))
    w_copies = []
    for j in range(KVH):
        columns = pl.ds(pl.multiple_of(head_of((j + 1) % n) * HD, HD), HD)
        for kind, w_hbm in enumerate((wk_hbm, wv_hbm)):
            w_copies.append(pltpu.make_async_copy(
                w_hbm.at[:, columns],
                weights.at[j, :, pl.ds(kind * HD, HD)],
                w_sem.at[0 if j else kind],
            ))
    off_copy = pltpu.make_async_copy(off_hbm, off_in, small_sem.at[1])
    q_copy = pltpu.make_async_copy(q_hbm, q_buf, small_sem.at[0])
    bias_copy = pltpu.make_async_copy(bias_hbm, bias_buf, x_sem.at[1])
    gain_copy.start()
    x_copies[0].start()
    w_copies[0].start()
    w_copies[1].start()
    for copy in x_copies[1:]:
        copy.start()
    off_copy.start()

    barrier = pltpu.get_barrier_semaphore()
    for d in order:
        pl.semaphore_signal(
            barrier, inc=1, device_id={"sp": lax.rem(me + d, n)}, device_id_type=MESH
        )

    gain_copy.wait()
    gain = gain_buf[...]

    def prepare(c):
        start, count = chunks[c]
        x_copies[c].wait()

        def step(i, _):
            rows = pl.ds(pl.multiple_of(start + i * STEP, STEP), STEP)
            x = x_buf[rows, :].astype(jnp.float32)
            scale = lax.rsqrt(jnp.mean(x * x, axis=-1, keepdims=True) + EPSILON)
            normed[rows, :] = (x * scale * gain).astype(jnp.bfloat16)
            return 0

        lax.fori_loop(0, count // STEP, step, 0, unroll=4)

    def later_loads():
        for copy in w_copies[2:]:
            copy.start()
        q_copy.start()

    def wait_weights(i):
        if i == 2 % n:
            part = weights.at[pl.ds(1, KVH - 1)]
            pltpu.make_async_copy(part, part, w_sem.at[0]).wait()

    def slot(i):
        if n == KVH:
            return (i - 1) % n
        first = head_of(1)
        down = lax.rem(first - head_of(i) + KVH, KVH)
        return jnp.where(lower, down, lax.rem(KVH - down, KVH))

    def project(i, start, count, columns):
        base = lax.div(peer(i), KVH) * block if seqs > 1 else 0
        rows = pl.ds(pl.multiple_of(base + start, STEP) if seqs > 1 else start, count)
        product = jnp.dot(
            normed[rows, :], weights[slot(i), :, columns], preferred_element_type=jnp.float32
        )
        return [
            product[:, c:c + HD].astype(jnp.bfloat16) for c in range(0, product.shape[1], HD)
        ]

    def prepare_and_project(start, count, columns):
        rows = pl.ds(start, count)
        squares = jnp.zeros((count, HD), jnp.float32)
        for c in range(0, width, HD):
            x = x_buf[rows, pl.ds(c, HD)].astype(jnp.float32)
            squares = squares + x * x
        scale = lax.rsqrt(jnp.sum(squares, axis=-1, keepdims=True) / width + EPSILON)
        if start == 0:
            w_copies[0].wait()
        product = jnp.zeros((count, columns.size), jnp.float32)
        for k in range(0, width, DEPTH):
            part = pl.ds(k, DEPTH)
            x = x_buf[rows, part].astype(jnp.float32)
            y = (x * scale * gain[:, k:k + DEPTH]).astype(jnp.bfloat16)
            normed[rows, part] = y
            product = product + jnp.dot(
                y, weights[slot(1), part, columns], preferred_element_type=jnp.float32
            )
        return [
            product[:, c:c + HD].astype(jnp.bfloat16) for c in range(0, columns.size, HD)
        ]

    def remote(src, dst, landed, target):
        return pltpu.make_async_remote_copy(
            src_ref=src, dst_ref=dst, send_sem=x_sem.at[0], recv_sem=landed,
            device_id={"sp": target}, device_id_type=MESH,
        )

    key_part, value_part = pl.ds(0, block), pl.ds(block, block)
    off_part = pl.ds(2 * block, unit - 2 * block)

    def copy_out(i, part, is_value=False):
        is_last = me == last_source(peer(i), n)
        sem = land_sem.at[jnp.where(is_last, 2 if is_value else 1, 0)]
        remote(sends.at[i - 1, part], land.at[me, part], sem, peer(i)).start()

    def lay_offsets():
        off_copy.wait()
        for s in range(seqs):
            values = off_in[s].astype(jnp.float32)
            for h in range(KVH):
                rows = [values[h:h + 1, c:c + HD] for c in range(0, block, HD)]
                blank = jnp.zeros((unit - 2 * block - len(rows), HD), jnp.float32)
                tile = jnp.concatenate(rows + [blank], axis=0)
                off_tiles[s * KVH + h] = tile.astype(jnp.bfloat16)
        for i in order:
            sends[i - 1, off_part] = off_tiles[peer(i)]
        land[me, off_part] = off_tiles[me]

    def greet():
        pl.semaphore_wait(barrier, n - 1)
        for i in order:
            copy_out(i, off_part)

    both = pl.ds(0, 2 * HD)
    if seqs > 1:
        lay_offsets()
    if seqs == 1:
        for c, (start, count) in enumerate(chunks):
            x_copies[c].wait()
            if c == len(chunks) - 1:
                later_loads()
            keys, values = pl.ds(start, count), pl.ds(block + start, count)
            if c == 0:
                sends[0, keys], = prepare_and_project(start, count, pl.ds(0, HD))
                pl.semaphore_wait(barrier, n - 1)
                copy_out(1, keys)
                lay_offsets()
                for i in order:
                    copy_out(i, off_part)
                w_copies[1].wait()
                sends[0, values], = project(1, start, count, pl.ds(HD, HD))
            else:
                sends[0, keys], sends[0, values] = prepare_and_project(start, count, both)
                copy_out(1, keys)
            copy_out(1, values, True)
    else:
        for c in range(len(chunks)):
            prepare(c)
        w_copies[0].wait()
        w_copies[1].wait()
        later_loads()
        sends[0, key_part], sends[0, value_part] = project(1, 0, block, both)
        greet()
        copy_out(1, key_part)
        copy_out(1, value_part, True)
    bias_copy.start()
    for i in order[1:]:
        wait_weights(i)
        sends[i - 1, key_part], sends[i - 1, value_part] = project(i, 0, block, both)
        if i > n // 2:
            copy_out(i, pl.ds(0, 2 * block))
        else:
            copy_out(i, key_part)
            copy_out(i, value_part, True)
    wait_weights(0)
    land[me, key_part], land[me, value_part] = project(0, 0, block, both)

    q_copy.wait()
    q_all = q_buf[0].astype(jnp.float32)
    q_rows = jnp.concatenate([q_all[:, g * HD:(g + 1) * HD] for g in range(GROUP)] * 2, axis=0)
    q_rows = q_rows.astype(jnp.bfloat16)
    bias_copy.wait()
    row_id = lax.broadcasted_iota(jnp.int32, (2 * GROUP, H), 0)
    lane_id = lax.broadcasted_iota(jnp.int32, (2 * GROUP, H), 1)
    chosen = lane_id == lax.rem(me, KVH) * GROUP + lax.rem(row_id, GROUP)
    bias = jnp.sum(jnp.where(chosen, bias_buf[...], 0.0), axis=1, keepdims=True)

    def arrived(part, sem):
        remote(part, part, sem, peer(1)).wait_recv()

    if n > 2:
        arrived(land.at[pl.ds(0, n - 2)], land_sem.at[0])
    arrived(land.at[0, pl.ds(block, unit - block)], land_sem.at[1])
    off_rows = []
    scores = []
    for source in range(n):
        tile = land[source, off_part].astype(jnp.float32)
        off_rows += [tile[c:c + 1] for c in range(block // HD)]
        scores.append(lax.dot_general(
            q_rows, land[source, key_part], (((1,), (1,)), ((), ())),
            preferred_element_type=jnp.float32,
        ))
    off_row = jnp.concatenate(off_rows, axis=1)
    off_out[0] = off_row.astype(jnp.bfloat16)
    scores = jnp.concatenate(scores, axis=1) / math.sqrt(HD) + bias + off_row
    tail = jnp.log1p(jnp.exp(-jnp.abs(scores)))
    spread = jnp.maximum(scores, 0.0) + tail
    log_sig = jnp.minimum(scores, 0.0) - tail
    pieces = length // HD
    cut = [spread[:, c * HD:(c + 1) * HD] for c in range(pieces)]
    stacked = jnp.concatenate(cut, axis=0)
    after = (
        lax.broadcasted_iota(jnp.int32, (HD, HD), 0) > lax.broadcasted_iota(jnp.int32, (HD, HD), 1)
    ).astype(jnp.float32)
    inner = jnp.dot(
        stacked, after, preferred_element_type=jnp.float32, precision=lax.Precision.HIGHEST
    )
    sums = jnp.sum(stacked, axis=1, keepdims=True)
    carried = jnp.zeros((2 * GROUP, 1), jnp.float32)
    for c in reversed(range(pieces)):
        rows = slice(c * 2 * GROUP, (c + 1) * 2 * GROUP)
        beyond = inner[rows] + carried
        stick[:, c * HD:(c + 1) * HD] = jnp.exp(log_sig[:, c * HD:(c + 1) * HD] - beyond)
        carried = carried + sums[rows]

    mixture = jnp.zeros((2 * GROUP, HD), jnp.float32)
    for j in range(n - 1):
        source = lax.rem(last_source(me, n) + 1 + j, n)
        mixture = mixture + read_block(stick, land, source, block)
    mix_out[...] = mixture
    remote(sends, sends, land_sem.at[0], peer(1)).wait_send()
    arrived(land.at[0, value_part], land_sem.at[2])


def read_block(stick, land, source, block):
    part = pl.ds(pl.multiple_of(source * block, block), block)
    return jnp.dot(
        stick[:, part].astype(jnp.bfloat16), land[source, pl.ds(block, block)],
        preferred_element_type=jnp.float32,
    )


def finish(n, land, off_in, stick, mix_in, k_out, v_out, off_out, read_out, read_buf, sem):
    block = k_out.shape[2] // n
    for source in range(n):
        there = pl.ds(source * block, block)
        for kind, cache in enumerate((k_out, v_out)):
            pltpu.make_async_copy(
                land.at[source, pl.ds(kind * block, block)], cache.at[0, 0, there], sem.at[0]
            ).start()
    off_copy = pltpu.make_async_copy(off_in, off_out, sem.at[1])
    off_copy.start()
    mixture = mix_in[...] + read_block(stick, land, last_source(lax.axis_index("sp"), n), block)
    scale = lax.rsqrt(jnp.mean(mixture * mixture, axis=-1, keepdims=True) + EPSILON)
    read = mixture * scale
    read_buf[0] = jnp.concatenate([read[g:g + 1] for g in range(GROUP)], axis=1).astype(jnp.bfloat16)
    read_copy = pltpu.make_async_copy(read_buf, read_out, sem.at[2])
    read_copy.start()
    caches = land.at[:, pl.ds(0, 2 * block)]
    pltpu.make_async_copy(caches, caches, sem.at[0]).wait()
    off_copy.wait()
    read_copy.wait()


def chunks_of(seqs, block):
    return tuple((r, ROWS) for r in range(0, seqs * block, ROWS))


def shards(layer_input, input_gain, key_weight, value_weight, stick_offsets, head_bias, queries):
    seqs, block, width = layer_input.shape
    n = lax.axis_size("sp")
    length = n * block
    total = seqs * block
    unit = unit_rows(block)
    hbm = pl.BlockSpec(memory_space=pltpu.HBM)
    vmem = pl.BlockSpec(memory_space=pltpu.VMEM)
    group_width = queries.shape[-1]
    chunks = chunks_of(seqs, block)
    cache = ((1, 1, length, HD), jnp.bfloat16)
    offsets = ((1, 1, length), jnp.bfloat16)
    read = ((1, 1, group_width), jnp.bfloat16)
    held_outs = (
        ((n, unit, HD), jnp.bfloat16),
        offsets,
        ((2 * GROUP, length), jnp.float32),
        ((2 * GROUP, HD), jnp.float32),
    )
    held = pl.pallas_call(
        functools.partial(kernel, n, seqs, chunks),
        out_shape=tuple(pltpu.VMEM(*out) for out in held_outs),
        in_specs=[hbm] * 7,
        out_specs=(vmem,) * len(held_outs),
        scratch_shapes=[
            pltpu.VMEM((total, width), jnp.bfloat16),
            pltpu.VMEM((total, width), jnp.bfloat16),
            pltpu.VMEM((KVH, width, 2 * HD), jnp.bfloat16),
            pltpu.VMEM((n - 1, unit, HD), jnp.bfloat16),
            pltpu.VMEM((1, width), jnp.float32),
            pltpu.VMEM((1, H), jnp.float32),
            pltpu.VMEM((seqs, KVH, block), jnp.bfloat16),
            pltpu.VMEM((n, unit - 2 * block, HD), jnp.bfloat16),
            pltpu.VMEM((1, 1, group_width), jnp.bfloat16),
            pltpu.SemaphoreType.DMA((len(chunks),)),
            pltpu.SemaphoreType.DMA((2,)),
            pltpu.SemaphoreType.DMA((2,)),
            pltpu.SemaphoreType.DMA((3,)),
        ],
        compiler_params=pltpu.CompilerParams(
            collective_id=0, has_side_effects=True, vmem_limit_bytes=VMEM_BYTES - 4 * length * HD - SPARE_BYTES
        ),
    )(
        layer_input.reshape(total, width),
        input_gain.reshape(1, width),
        key_weight,
        value_weight,
        jnp.transpose(stick_offsets, (1, 0, 2)),
        head_bias.reshape(1, H),
        queries,
    )
    outs = (cache, cache, offsets, read)
    return pl.pallas_call(
        functools.partial(finish, n),
        out_shape=tuple(jax.ShapeDtypeStruct(*out) for out in outs),
        in_specs=[vmem] * len(held_outs),
        out_specs=(hbm,) * len(outs),
        scratch_shapes=[
            pltpu.VMEM(*read),
            pltpu.SemaphoreType.DMA((3,)),
        ],
        compiler_params=pltpu.CompilerParams(vmem_limit_bytes=WRITE_BYTES),
    )(*held)


def solution(mesh):
    placed = (
        P(("grp", "tp"), "sp", None),
        P(),
        P(),
        P(),
        P(None, ("grp", "tp"), "sp"),
        P(),
        P(("grp", "tp"), "sp", None),
    )
    return jax.shard_map(
        shards,
        mesh=mesh,
        in_specs=placed,
        out_specs=(
            P(("grp", "tp"), "sp", None, None),
            P(("grp", "tp"), "sp", None, None),
            P(("grp", "tp"), "sp", None),
            P(("grp", "tp"), "sp", None),
        ),
        check_vma=False,
    )
```

```python
import functools
import math

import jax
import jax.numpy as jnp
from jax import lax
from jax.experimental import pallas as pl
from jax.experimental.pallas import tpu as pltpu
from jax.sharding import PartitionSpec as P

H = 16
KVH = 4
HD = 128
GROUP = H // KVH
EPSILON = 1e-06
ROWS = 128
STEP = 16
TILE = 8
DEPTH = 1024
VMEM_BYTES = 67043328
SPARE_BYTES = 524288
WRITE_BYTES = 1048576
MESH = pl.DeviceIdType.MESH


def last_source(me, n):
    return jnp.where(2 * me < n, n // 2, n // 2 - 1)


def unit_rows(block):
    return 2 * block + -(-block // (HD * TILE)) * TILE


def kernel(
    n, seqs, chunks, x_hbm, gain_hbm, wk_hbm, wv_hbm, off_hbm, bias_hbm, q_hbm,
    land, off_out, stick, mix_out,
    x_buf, scaled, row_scale, weights, sends, gain_buf, bias_buf, off_in, off_tiles, q_buf,
    x_sem, w_sem, small_sem, land_sem,
):
    total, width = x_buf.shape
    block = total // seqs
    length = n * block
    unit = unit_rows(block)
    me = lax.axis_index("sp")
    order = range(1, n)
    lower = 2 * me < n
    near = jnp.where(lower, me, n - 1 - me)

    def peer(i):
        if i == 0:
            return me
        if i == 1:
            return jnp.where(lower, n - 1, 0)
        far = jnp.where(i <= n - 1 - near, n - i, n - 1 - i)
        return jnp.where(lower, far, n - 1 - far)

    def head_of(i):
        return lax.rem(peer(i), KVH)

    gain_copy = pltpu.make_async_copy(gain_hbm, gain_buf, small_sem.at[0])
    x_copies = []
    for c, (start, rows) in enumerate(chunks):
        part = pl.ds(start, rows)
        x_copies.append(pltpu.make_async_copy(x_hbm.at[part], x_buf.at[part], x_sem.at[c]))
    w_copies = []
    for j in range(KVH):
        columns = pl.ds(pl.multiple_of(head_of((j + 1) % n) * HD, HD), HD)
        for kind, w_hbm in enumerate((wk_hbm, wv_hbm)):
            w_copies.append(pltpu.make_async_copy(
                w_hbm.at[:, columns],
                weights.at[j, :, pl.ds(kind * HD, HD)],
                w_sem.at[0 if j else kind],
            ))
    off_copy = pltpu.make_async_copy(off_hbm, off_in, small_sem.at[1])
    q_copy = pltpu.make_async_copy(q_hbm, q_buf, small_sem.at[0])
    bias_copy = pltpu.make_async_copy(bias_hbm, bias_buf, x_sem.at[1])
    gain_copy.start()
    x_copies[0].start()
    w_copies[0].start()
    w_copies[1].start()
    for copy in x_copies[1:]:
        copy.start()
    off_copy.start()

    barrier = pltpu.get_barrier_semaphore()
    for d in order:
        pl.semaphore_signal(
            barrier, inc=1, device_id={"sp": lax.rem(me + d, n)}, device_id_type=MESH
        )

    gain_copy.wait()
    gain = gain_buf[...]

    def prepare(c):
        start, count = chunks[c]
        x_copies[c].wait()

        def step(i, _):
            rows = pl.ds(pl.multiple_of(start + i * STEP, STEP), STEP)
            x = x_buf[rows, :].astype(jnp.float32)
            scaled[rows, :] = (x * gain).astype(jnp.bfloat16)
            scale = lax.rsqrt(jnp.mean(x * x, axis=-1, keepdims=True) + EPSILON)
            row_scale[rows, :] = jnp.broadcast_to(scale, (STEP, HD))
            return 0

        lax.fori_loop(0, count // STEP, step, 0, unroll=4)

    def later_loads():
        for copy in w_copies[2:]:
            copy.start()
        q_copy.start()

    def wait_weights(i):
        if i == 2 % n:
            part = weights.at[pl.ds(1, KVH - 1)]
            pltpu.make_async_copy(part, part, w_sem.at[0]).wait()

    def slot(i):
        if n == KVH:
            return (i - 1) % n
        first = head_of(1)
        down = lax.rem(first - head_of(i) + KVH, KVH)
        return jnp.where(lower, down, lax.rem(KVH - down, KVH))

    def project(i, start, count, columns):
        base = lax.div(peer(i), KVH) * block if seqs > 1 else 0
        rows = pl.ds(pl.multiple_of(base + start, STEP) if seqs > 1 else start, count)
        product = jnp.dot(
            scaled[rows, :], weights[slot(i), :, columns], preferred_element_type=jnp.float32
        )
        scale = row_scale[rows, :]
        return [
            (product[:, c:c + HD] * scale).astype(jnp.bfloat16)
            for c in range(0, product.shape[1], HD)
        ]

    def prepare_and_project(start, count, columns):
        rows = pl.ds(start, count)
        product = jnp.zeros((count, columns.size), jnp.float32)
        squares = jnp.zeros((count, HD), jnp.float32)
        for k in range(0, width, DEPTH):
            part = pl.ds(k, DEPTH)
            x = x_buf[rows, part].astype(jnp.float32)
            y = (x * gain[:, k:k + DEPTH]).astype(jnp.bfloat16)
            scaled[rows, part] = y
            for c in range(0, DEPTH, HD):
                squares = squares + x[:, c:c + HD] * x[:, c:c + HD]
            product = product + jnp.dot(
                y, weights[slot(1), part, columns], preferred_element_type=jnp.float32
            )
        scale = lax.rsqrt(jnp.sum(squares, axis=-1, keepdims=True) / width + EPSILON)
        scale = jnp.broadcast_to(scale, (count, HD))
        row_scale[rows, :] = scale
        return [
            (product[:, c:c + HD] * scale).astype(jnp.bfloat16)
            for c in range(0, columns.size, HD)
        ]

    def remote(src, dst, landed, target):
        return pltpu.make_async_remote_copy(
            src_ref=src, dst_ref=dst, send_sem=x_sem.at[0], recv_sem=landed,
            device_id={"sp": target}, device_id_type=MESH,
        )

    key_part, value_part = pl.ds(0, block), pl.ds(block, block)
    off_part = pl.ds(2 * block, unit - 2 * block)

    def copy_out(i, part, is_value=False):
        is_last = me == last_source(peer(i), n)
        sem = land_sem.at[jnp.where(is_last, 2 if is_value else 1, 0)]
        remote(sends.at[i - 1, part], land.at[me, part], sem, peer(i)).start()

    def lay_offsets():
        off_copy.wait()
        for s in range(seqs):
            values = off_in[s].astype(jnp.float32)
            for h in range(KVH):
                rows = [values[h:h + 1, c:c + HD] for c in range(0, block, HD)]
                blank = jnp.zeros((unit - 2 * block - len(rows), HD), jnp.float32)
                tile = jnp.concatenate(rows + [blank], axis=0)
                off_tiles[s * KVH + h] = tile.astype(jnp.bfloat16)
        for i in order:
            sends[i - 1, off_part] = off_tiles[peer(i)]
        land[me, off_part] = off_tiles[me]

    def greet():
        pl.semaphore_wait(barrier, n - 1)
        for i in order:
            copy_out(i, off_part)

    both = pl.ds(0, 2 * HD)
    if seqs > 1:
        lay_offsets()
    if seqs == 1:
        for c, (start, count) in enumerate(chunks):
            x_copies[c].wait()
            if c == len(chunks) - 1:
                later_loads()
            keys, values = pl.ds(start, count), pl.ds(block + start, count)
            if c == 0:
                w_copies[0].wait()
                sends[0, keys], = prepare_and_project(start, count, pl.ds(0, HD))
                pl.semaphore_wait(barrier, n - 1)
                copy_out(1, keys)
                lay_offsets()
                for i in order:
                    copy_out(i, off_part)
                w_copies[1].wait()
                sends[0, values], = project(1, start, count, pl.ds(HD, HD))
            else:
                sends[0, keys], sends[0, values] = prepare_and_project(start, count, both)
                copy_out(1, keys)
            copy_out(1, values, True)
    else:
        for c in range(len(chunks)):
            prepare(c)
        w_copies[0].wait()
        w_copies[1].wait()
        later_loads()
        sends[0, key_part], sends[0, value_part] = project(1, 0, block, both)
        greet()
        copy_out(1, key_part)
        copy_out(1, value_part, True)
    bias_copy.start()
    for i in order[1:]:
        wait_weights(i)
        sends[i - 1, key_part], sends[i - 1, value_part] = project(i, 0, block, both)
        if i > n // 2:
            copy_out(i, pl.ds(0, 2 * block))
        else:
            copy_out(i, key_part)
            copy_out(i, value_part, True)
    wait_weights(0)
    land[me, key_part], land[me, value_part] = project(0, 0, block, both)

    q_copy.wait()
    q_all = q_buf[0].astype(jnp.float32)
    q_rows = jnp.concatenate([q_all[:, g * HD:(g + 1) * HD] for g in range(GROUP)] * 2, axis=0)
    q_rows = q_rows.astype(jnp.bfloat16)
    bias_copy.wait()
    row_id = lax.broadcasted_iota(jnp.int32, (2 * GROUP, H), 0)
    lane_id = lax.broadcasted_iota(jnp.int32, (2 * GROUP, H), 1)
    chosen = lane_id == lax.rem(me, KVH) * GROUP + lax.rem(row_id, GROUP)
    bias = jnp.sum(jnp.where(chosen, bias_buf[...], 0.0), axis=1, keepdims=True)

    def arrived(part, sem):
        remote(part, part, sem, peer(1)).wait_recv()

    if n > 2:
        arrived(land.at[pl.ds(0, n - 2)], land_sem.at[0])
    arrived(land.at[0, pl.ds(block, unit - block)], land_sem.at[1])
    off_rows = []
    scores = []
    for source in range(n):
        tile = land[source, off_part].astype(jnp.float32)
        off_rows += [tile[c:c + 1] for c in range(block // HD)]
        scores.append(lax.dot_general(
            q_rows, land[source, key_part], (((1,), (1,)), ((), ())),
            preferred_element_type=jnp.float32,
        ))
    off_row = jnp.concatenate(off_rows, axis=1)
    off_out[0] = off_row.astype(jnp.bfloat16)
    scores = jnp.concatenate(scores, axis=1) / math.sqrt(HD) + bias + off_row
    tail = jnp.log1p(jnp.exp(-jnp.abs(scores)))
    spread = jnp.maximum(scores, 0.0) + tail
    log_sig = jnp.minimum(scores, 0.0) - tail
    pieces = length // HD
    cut = [spread[:, c * HD:(c + 1) * HD] for c in range(pieces)]
    stacked = jnp.concatenate(cut, axis=0)
    after = (
        lax.broadcasted_iota(jnp.int32, (HD, HD), 0) > lax.broadcasted_iota(jnp.int32, (HD, HD), 1)
    ).astype(jnp.float32)
    inner = jnp.dot(
        stacked, after, preferred_element_type=jnp.float32, precision=lax.Precision.HIGHEST
    )
    sums = jnp.sum(stacked, axis=1, keepdims=True)
    carried = jnp.zeros((2 * GROUP, 1), jnp.float32)
    for c in reversed(range(pieces)):
        rows = slice(c * 2 * GROUP, (c + 1) * 2 * GROUP)
        beyond = inner[rows] + carried
        stick[:, c * HD:(c + 1) * HD] = jnp.exp(log_sig[:, c * HD:(c + 1) * HD] - beyond)
        carried = carried + sums[rows]

    mixture = jnp.zeros((2 * GROUP, HD), jnp.float32)
    for j in range(n - 1):
        source = lax.rem(last_source(me, n) + 1 + j, n)
        mixture = mixture + read_block(stick, land, source, block)
    mix_out[...] = mixture
    remote(sends, sends, land_sem.at[0], peer(1)).wait_send()
    arrived(land.at[0, value_part], land_sem.at[2])


def read_block(stick, land, source, block):
    part = pl.ds(pl.multiple_of(source * block, block), block)
    return jnp.dot(
        stick[:, part].astype(jnp.bfloat16), land[source, pl.ds(block, block)],
        preferred_element_type=jnp.float32,
    )


def finish(n, land, off_in, stick, mix_in, k_out, v_out, off_out, read_out, read_buf, sem):
    block = k_out.shape[2] // n
    for source in range(n):
        there = pl.ds(source * block, block)
        for kind, cache in enumerate((k_out, v_out)):
            pltpu.make_async_copy(
                land.at[source, pl.ds(kind * block, block)], cache.at[0, 0, there], sem.at[0]
            ).start()
    off_copy = pltpu.make_async_copy(off_in, off_out, sem.at[1])
    off_copy.start()
    mixture = mix_in[...] + read_block(stick, land, last_source(lax.axis_index("sp"), n), block)
    scale = lax.rsqrt(jnp.mean(mixture * mixture, axis=-1, keepdims=True) + EPSILON)
    read = mixture * scale
    read_buf[0] = jnp.concatenate([read[g:g + 1] for g in range(GROUP)], axis=1).astype(jnp.bfloat16)
    read_copy = pltpu.make_async_copy(read_buf, read_out, sem.at[2])
    read_copy.start()
    caches = land.at[:, pl.ds(0, 2 * block)]
    pltpu.make_async_copy(caches, caches, sem.at[0]).wait()
    off_copy.wait()
    read_copy.wait()


def chunks_of(seqs, block):
    return tuple((r, ROWS) for r in range(0, seqs * block, ROWS))


def shards(layer_input, input_gain, key_weight, value_weight, stick_offsets, head_bias, queries):
    seqs, block, width = layer_input.shape
    n = lax.axis_size("sp")
    length = n * block
    total = seqs * block
    unit = unit_rows(block)
    hbm = pl.BlockSpec(memory_space=pltpu.HBM)
    vmem = pl.BlockSpec(memory_space=pltpu.VMEM)
    group_width = queries.shape[-1]
    chunks = chunks_of(seqs, block)
    cache = ((1, 1, length, HD), jnp.bfloat16)
    offsets = ((1, 1, length), jnp.bfloat16)
    read = ((1, 1, group_width), jnp.bfloat16)
    held_outs = (
        ((n, unit, HD), jnp.bfloat16),
        offsets,
        ((2 * GROUP, length), jnp.float32),
        ((2 * GROUP, HD), jnp.float32),
    )
    held = pl.pallas_call(
        functools.partial(kernel, n, seqs, chunks),
        out_shape=tuple(pltpu.VMEM(*out) for out in held_outs),
        in_specs=[hbm] * 7,
        out_specs=(vmem,) * len(held_outs),
        scratch_shapes=[
            pltpu.VMEM((total, width), jnp.bfloat16),
            pltpu.VMEM((total, width), jnp.bfloat16),
            pltpu.VMEM((total, HD), jnp.float32),
            pltpu.VMEM((KVH, width, 2 * HD), jnp.bfloat16),
            pltpu.VMEM((n - 1, unit, HD), jnp.bfloat16),
            pltpu.VMEM((1, width), jnp.float32),
            pltpu.VMEM((1, H), jnp.float32),
            pltpu.VMEM((seqs, KVH, block), jnp.bfloat16),
            pltpu.VMEM((n, unit - 2 * block, HD), jnp.bfloat16),
            pltpu.VMEM((1, 1, group_width), jnp.bfloat16),
            pltpu.SemaphoreType.DMA((len(chunks),)),
            pltpu.SemaphoreType.DMA((2,)),
            pltpu.SemaphoreType.DMA((2,)),
            pltpu.SemaphoreType.DMA((3,)),
        ],
        compiler_params=pltpu.CompilerParams(
            collective_id=0, has_side_effects=True, vmem_limit_bytes=VMEM_BYTES - 4 * length * HD - SPARE_BYTES
        ),
    )(
        layer_input.reshape(total, width),
        input_gain.reshape(1, width),
        key_weight,
        value_weight,
        jnp.transpose(stick_offsets, (1, 0, 2)),
        head_bias.reshape(1, H),
        queries,
    )
    outs = (cache, cache, offsets, read)
    return pl.pallas_call(
        functools.partial(finish, n),
        out_shape=tuple(jax.ShapeDtypeStruct(*out) for out in outs),
        in_specs=[vmem] * len(held_outs),
        out_specs=(hbm,) * len(outs),
        scratch_shapes=[
            pltpu.VMEM(*read),
            pltpu.SemaphoreType.DMA((3,)),
        ],
        compiler_params=pltpu.CompilerParams(vmem_limit_bytes=WRITE_BYTES),
    )(*held)


def solution(mesh):
    placed = (
        P(("grp", "tp"), "sp", None),
        P(),
        P(),
        P(),
        P(None, ("grp", "tp"), "sp"),
        P(),
        P(("grp", "tp"), "sp", None),
    )
    return jax.shard_map(
        shards,
        mesh=mesh,
        in_specs=placed,
        out_specs=(
            P(("grp", "tp"), "sp", None, None),
            P(("grp", "tp"), "sp", None, None),
            P(("grp", "tp"), "sp", None),
            P(("grp", "tp"), "sp", None),
        ),
        check_vma=False,
    )
```
